512 devices in a mesh: fs: 128 (over z, y, core), tp: 4 (over x).
Axes of the slice: x: 4, y: 8, z: 8, core: 2. Of those that a mesh axis runs over, the one named last changes fastest.
Arguments:
- tokens: bfloat16 [16384, 2048], P('fs', 'tp'), may hold values from -6 to 6
- routes: int32 [16384, 2], P('fs'), may hold values from 0 to 127, all different within a row; in each aligned block of 128 rows (0 to 127, 128 to 255, ...) at most 3 rows name the same one
- route_weight: float32 [16384, 2], P('fs'), may hold values from 0.05 to 1
- gain: float32 [2048], P('fs'), may hold values from 0.1 to 1.9
- gate_weight: float32 [128, 2048, 512], P(None, 'fs', 'tp'), may hold values from -0.125 to 0.125
- up_weight: float32 [128, 2048, 512], P(None, 'fs', 'tp'), may hold values from -0.125 to 0.125
- down_weight: float32 [128, 512, 2048], P(None, 'tp', 'fs'), may hold values from -0.25 to 0.25
Outputs:
- gate_out: bfloat16 [128, 2048, 512], P('fs', None, 'tp')
- up_out: bfloat16 [128, 2048, 512], P('fs', None, 'tp')
- down_out: bfloat16 [128, 512, 2048], P('fs', 'tp')
- mixed: bfloat16 [16384, 2048], P('fs', 'tp')
The draws below stay inside these ranges and needn't reach their ends.
Inputs may be any that keep to these rules, and one draw needn't show every extreme that they name: `routes`: each row names 2 different experts. Among the rows of one index of fs (aligned blocks of 128 rows) no expert is named more than 3 times, a bound that some block reaches.
All inputs are finite; a program needn't handle non-finite values.
Results may differ from the reference program's by a relative error of at most 0.0095.
Values may be sent and summed in bfloat16 or wider, within the bound.
No kernel may reach another device: no remote copies, remote signals or barrier semaphores. Data moves between devices by JAX's collectives and lax.ppermute only.
A program may use at most 64 MiB of HBM per device.

```python
import math
import jax
import jax.numpy as jnp
import numpy as np
from jax import lax

D = 2048
F = 512
TOP = 2
TOK_DEV = 128
EXPERTS = 128
CAP = 3
TOKENS = 16384
N_FS = 128
N_TP = 4


def block_scale(rng, shape, cuts, smallest, high):
    loudness = 1.0
    for dim, blocks in cuts:
        heights = jax.random.uniform(jax.random.fold_in(jax.random.fold_in(rng, 6), dim), (blocks,), jnp.float32, smallest / len(cuts), high / len(cuts))
        loudness = loudness * jnp.repeat(jnp.exp(heights), shape[dim] // blocks).reshape((-1,) + (1,) * (len(shape) - 1 - dim))
    return loudness


def shared_out(own_key, own, number, rows, count, top, limit, lean):
    sequence = jax.random.permutation(own_key, count)
    heavy_load, usual = shares(count, rows * top, limit, lean, True), shares(count, rows * top, limit, lean, False)
    places = jnp.arange(count)

    def named(sizes, rotation):
        used = int((sizes > 0).sum())
        fixed = max(1, used // 4)
        moved = fixed + (places - fixed + rotation * (used - fixed)) % max(1, count - fixed)
        return jnp.zeros((count,), jnp.int32).at[sequence[jnp.where(places < fixed, places, moved)]].set(jnp.asarray(sizes, jnp.int32))

    sizes = jnp.where(number % 4 == 0, named(heavy_load, number // 4), named(usual, number - number // 4 - 1))
    mixed = jax.random.permutation(jax.random.fold_in(own, 3), count)
    source_of, taker = mixed[0:count // 2 * 2:2], mixed[1:count // 2 * 2:2]
    slack = jnp.minimum(sizes[source_of] - 1, limit - sizes[taker]) // 2
    slack = jnp.where((source_of == sequence[0]) | (taker == sequence[0]) | (sizes[taker] == 0), 0, jnp.maximum(slack, 0))
    moved = jax.random.randint(jax.random.fold_in(own, 4), (count // 2,), 0, 1 << 20) % (slack + 1)
    sizes = sizes.at[source_of].add(-moved).at[taker].add(moved)
    members = jnp.searchsorted(jnp.cumsum(sizes), jnp.arange(rows * top), side="right").astype(jnp.int32)
    table = members.reshape(top, rows).T
    table = table[jax.random.permutation(jax.random.fold_in(own, 1), rows)]
    rotation = jax.random.randint(jax.random.fold_in(own, 2), (rows, 1), 0, top)
    return jnp.take_along_axis(table, (jnp.arange(top)[None, :] + rotation) % top, axis=1)


def shares(amount, total, limit, skew, full):
    weights = [(1 << 20) // math.isqrt(standing ** skew) + 1 for standing in range(1, amount + 1)]
    largest = limit if full else min(limit, max(-(-total // amount), total * weights[0] // sum(weights)))
    least = 1 if total - largest >= amount - 1 else 0
    holding, spare = [largest] + [least] * (amount - 1), total - largest - least * (amount - 1)
    while spare > 0:
        movable = [i for i in range(1, amount) if holding[i] < largest] or [i for i in range(1, amount) if holding[i] < limit]
        mass, remaining = sum([weights[i] for i in movable]), spare
        for i in movable:
            extra = min(limit - holding[i], max(1, remaining * weights[i] // mass), spare)
            holding[i] = holding[i] + extra
            spare = spare - extra
    return np.array(holding)


def gaussian(own_key, dims, width, limit, split=(), kind=jnp.bfloat16):
    factor_of = block_scale(own_key, dims, split, -0.22, 0.18) if split else 1.0
    entries = jax.random.normal(own_key, dims, jnp.float32) * width * factor_of
    return jnp.minimum(jnp.maximum(entries, -limit), limit).astype(kind)


def setup_inputs(seed: int = 0) -> dict:
    seeds = jax.random.split(jax.random.key(seed), 8)
    tokens = gaussian(seeds[0], (TOKENS, D), 1.0, 6.0, ((0, 128), (1, 4)))
    routes_keys = jax.random.split(jax.random.fold_in(seeds[1], 1), TOKENS // TOK_DEV)
    routes_turns = jax.random.permutation(jax.random.fold_in(seeds[1], 3), TOKENS // TOK_DEV)
    routes = jax.vmap(lambda own, number: shared_out(jax.random.fold_in(seeds[1], 2), own, number, TOK_DEV, EXPERTS, TOP, CAP, 2))(routes_keys, routes_turns).reshape((TOKENS, TOP))
    route_weight = jnp.clip(0.05 + 0.95 * jax.random.uniform(seeds[2], (TOKENS, TOP), jnp.float32) ** block_scale(seeds[2], (TOKENS, TOP), ((0, 128),), -0.2, 0.2), 0.05, 1.0)
    gain = jnp.clip(1.0 + 0.18 * jax.random.normal(seeds[3], (D,), jnp.float32), 0.1, 1.9)
    gate_weight = gaussian(seeds[4], (EXPERTS, D, F), D ** -0.5, 0.125, ((1, 128), (2, 4)), jnp.float32)
    up_weight = gaussian(seeds[5], (EXPERTS, D, F), D ** -0.5, 0.125, ((1, 128), (2, 4)), jnp.float32)
    down_weight = gaussian(seeds[6], (EXPERTS, F, D), F ** -0.5, 0.25, ((1, 4), (2, 128)), jnp.float32)
    return dict(tokens=tokens, routes=routes, route_weight=route_weight, gain=gain, gate_weight=gate_weight, up_weight=up_weight, down_weight=down_weight)


def reference(tokens, routes, route_weight, gain, gate_weight, up_weight, down_weight):
    gate_out = (gain[None, :, None] * gate_weight).astype(jnp.bfloat16)
    up_out = (gain[None, :, None] * up_weight).astype(jnp.bfloat16)
    down_out = down_weight.astype(jnp.bfloat16)
    values = tokens.astype(jnp.float32)
    normed = (values * lax.rsqrt(lax.optimization_barrier(jnp.mean(values * values, axis=-1, keepdims=True)) + 1e-06)).astype(jnp.bfloat16)
    blocks = routes.reshape(N_FS, TOK_DEV * TOP)
    hits = (blocks[:, :, None] == jnp.arange(EXPERTS, dtype=jnp.int32)[None, None, :]).astype(jnp.int32)
    ranks = lax.optimization_barrier(jnp.sum((jnp.cumsum(hits, axis=1) - 1) * hits, axis=2))
    homes = jnp.arange(N_FS, dtype=jnp.int32)[:, None]
    position = (blocks * (N_FS * CAP) + homes * CAP + ranks).reshape(-1).astype(jnp.int32)
    count = TOKENS * TOP
    source = jnp.full((EXPERTS * N_FS * CAP,), count, jnp.int32)
    source = source.at[position].set(jnp.arange(count, dtype=jnp.int32)).reshape(EXPERTS, N_FS * CAP)
    unit = F // N_TP

    def per_expert(items):
        src, w_gate, w_up, w_down = items
        rows = normed[jnp.minimum(src // TOP, TOKENS - 1)]
        rows = jnp.where((src < count)[:, None], rows, jnp.zeros_like(rows))
        gate_act = jnp.dot(rows, w_gate, preferred_element_type=jnp.float32)
        up_act = jnp.dot(rows, w_up, preferred_element_type=jnp.float32)
        hidden = (jax.nn.silu(gate_act) * up_act).astype(jnp.bfloat16)
        pieces = []
        for block in range(N_TP):
            part = jnp.dot(hidden[:, block * unit:(block + 1) * unit], w_down[block * unit:(block + 1) * unit], preferred_element_type=jnp.float32).astype(jnp.bfloat16)
            pieces.append(part.astype(jnp.float32))
        return lax.optimization_barrier(jnp.sum(jnp.stack(pieces), axis=0)).astype(jnp.bfloat16)
    results = lax.map(per_expert, (source, gate_out, up_out, down_out))
    picked = results.reshape(EXPERTS * N_FS * CAP, D)[position].astype(jnp.float32).reshape(TOKENS, TOP, D)
    share = route_weight / lax.optimization_barrier(jnp.sum(route_weight, axis=1, keepdims=True))
    mixed = lax.optimization_barrier(jnp.sum(share[:, :, None] * picked, axis=1)).astype(jnp.bfloat16)
    return (gate_out, up_out, down_out, mixed)
```

```python
import jax
import jax.numpy as jnp
from jax import lax
from jax.experimental import pallas as pl
from jax.experimental.pallas import tpu as pltpu
from jax.sharding import PartitionSpec as P

SLOTS = 3
BF = jnp.bfloat16
F32 = jnp.float32


def vmem(count):
    return [pl.BlockSpec(memory_space=pltpu.VMEM)] * count


def slot_hits(routes):
    experts = lax.axis_size("fs")
    count = routes.shape[1]
    expert = lax.broadcasted_iota(jnp.int32, (experts, count), 0)
    first = routes[0:1, :] == expert
    second = routes[1:2, :] == expert
    hit = jnp.where(first | second, 1.0, 0.0)
    before = lax.broadcasted_iota(jnp.int32, (count, count), 0) < lax.broadcasted_iota(
        jnp.int32, (count, count), 1
    )
    order = jnp.dot(hit.astype(BF), jnp.where(before, 1.0, 0.0).astype(BF), preferred_element_type=F32)
    return first, hit, order


def pack_kernel(routes_ref, tokens_ref, down_ref, out_ref):
    _, hit, order = slot_hits(routes_ref[...])
    tokens = tokens_ref[...]
    experts = out_ref.shape[0]
    for s in range(SLOTS):
        chosen = jnp.where((hit > 0.0) & (order == float(s)), 1.0, 0.0).astype(BF)
        rows = jnp.dot(chosen, tokens, preferred_element_type=F32)
        out_ref[:, :, s * 128 : (s + 1) * 128] = rows.reshape(experts, 4, 128).astype(BF)
    base = SLOTS * 128
    for k in range(4):
        out_ref[:, :, base + k * 128 : base + (k + 1) * 128] = down_ref[:, 4 * k : 4 * k + 4, :].astype(BF)


def unpack_kernel(place_ref, got_ref, rows_ref, *down_refs):
    sources = got_ref.shape[0]
    for s in range(SLOTS):
        block = got_ref[:, :, s * 128 : (s + 1) * 128].astype(F32)
        rows_ref[s * sources : (s + 1) * sources, :] = block.reshape(sources, 512).astype(BF)
    base = SLOTS * 128
    part = sources // 4
    for shift, ref in enumerate(down_refs):
        start = ((place_ref[0] + shift) % 4) * part
        for k in range(4):
            ref[:, 4 * k : 4 * k + 4, :] = got_ref[
                pl.ds(start, part), :, base + k * 128 : base + (k + 1) * 128
            ]


def down_kernel(got_ref, out_ref):
    sources = got_ref.shape[0]
    base = SLOTS * 128
    parts = [got_ref[:, :, base + k * 128 : base + (k + 1) * 128] for k in range(4)]
    block = jnp.concatenate([p.astype(F32) for p in parts], axis=1)
    out_ref[...] = block.reshape(sources * 16, 128).T.astype(BF)


def norm_kernel(*refs):
    ins, outs = refs[:4], refs[4]
    values = [r[...].astype(F32) for r in ins]
    total = sum(jnp.sum(v * v, axis=1, keepdims=True) for v in values)
    scale = lax.rsqrt(total / 2048.0 + 1e-06)
    for k in range(4):
        outs[k] = (values[k] * scale).astype(BF)


def hidden_kernel(place_ref, rows_ref, weight_ref, out_ref):
    acc = None
    for k in range(4):
        block = (place_ref[0] + 4 - k) % 4
        part = jnp.dot(rows_ref[k], weight_ref[block], preferred_element_type=F32)
        acc = part if acc is None else acc + part
    gate = acc[:, :128]
    up = acc[:, 128:]
    out_ref[...] = (gate / (1.0 + jnp.exp(-gate)) * up).astype(BF)


def expert_kernel(place_ref, hidden_ref, d0, d1, d2, d3, out_ref):
    acc = None
    for k, ref in enumerate((d0, d1, d2, d3)):
        block = (place_ref[0] + 4 - k) % 4
        part = lax.dot_general(
            hidden_ref[block], ref[...], (((1,), (1,)), ((), ())), preferred_element_type=F32
        )
        acc = part if acc is None else acc + part
    sources = out_ref.shape[0]
    for s in range(SLOTS):
        rows = acc[s * sources : (s + 1) * sources, :].astype(BF).astype(F32)
        out_ref[:, :, s * 128 : (s + 1) * 128] = rows.reshape(sources, 4, 128).astype(BF)


def share_kernel(routes_ref, weight_ref, high_ref, low_ref):
    first, hit, order = slot_hits(routes_ref[...])
    weight = weight_ref[...]
    share = weight / jnp.sum(weight, axis=0, keepdims=True)
    mine = jnp.where(first, share[0:1, :], share[1:2, :])
    for s in range(SLOTS):
        part = jnp.where((hit > 0.0) & (order == float(s)), mine, 0.0).T
        high = part.astype(BF)
        high_ref[s] = high
        low_ref[s] = (part - high.astype(F32)).astype(BF)


def mix_kernel(high_ref, low_ref, back_ref, out_ref):
    experts = back_ref.shape[0]
    acc = None
    for s in range(SLOTS):
        rows = back_ref[:, :, s * 128 : (s + 1) * 128].astype(F32).reshape(experts, 512).astype(BF)
        part = jnp.dot(high_ref[s], rows, preferred_element_type=F32)
        part = part + jnp.dot(low_ref[s], rows, preferred_element_type=F32)
        acc = part if acc is None else acc + part
    out_ref[...] = acc.astype(BF)


def local(tokens, routes, route_weight, gain, gate_weight, up_weight, down_weight):
    place = lax.axis_index("tp").astype(jnp.int32).reshape(1)
    fs = lax.axis_size("fs")
    count = tokens.shape[0]
    wide = SLOTS * 128 + 512
    scalar = pl.BlockSpec(memory_space=pltpu.SMEM)
    routes = routes.T
    route_weight = route_weight.T

    packed = pl.pallas_call(
        pack_kernel, out_shape=jax.ShapeDtypeStruct((fs, 4, wide), BF), name="pack"
    )(routes, tokens, jnp.transpose(down_weight, (0, 2, 1)))
    got = lax.all_to_all(packed, "fs", 0, 0, tiled=True)

    gain_rows = gain[None, :, None]
    gate_new = (gain_rows * gate_weight).astype(BF)
    up_new = (gain_rows * up_weight).astype(BF)
    both = lax.all_to_all(jnp.concatenate((gate_new, up_new), axis=2), "fs", 0, 0, tiled=True)

    part = jax.ShapeDtypeStruct((fs // 4, 16, 128), BF)
    rows, *downs = pl.pallas_call(
        unpack_kernel,
        out_shape=(jax.ShapeDtypeStruct((SLOTS * fs, 512), BF), part, part, part, part),
        in_specs=[scalar] + vmem(1),
        name="unpack",
    )(place, got)

    def shifted(value, k):
        return lax.ppermute(value, "tp", [(i, (i + k) % 4) for i in range(4)])

    row_parts = [rows, None, None, None]
    down_parts = [downs[0], None, None, None]
    for k in (1, 3, 2):
        row_parts[k] = shifted(rows, k)
    for k in (1, 3, 2):
        down_parts[k] = shifted(downs[k], k)
    normed = pl.pallas_call(
        norm_kernel, out_shape=jax.ShapeDtypeStruct((4, SLOTS * fs, 512), BF), name="norm"
    )(*row_parts)

    hidden = pl.pallas_call(
        hidden_kernel,
        out_shape=jax.ShapeDtypeStruct((SLOTS * fs, 128), BF),
        in_specs=[scalar] + vmem(2),
        name="hidden",
    )(place, normed, both.reshape(4, 512, 256))
    hidden = lax.all_gather(hidden, "tp", axis=0, tiled=False)
    result = pl.pallas_call(
        expert_kernel,
        out_shape=jax.ShapeDtypeStruct((fs, 4, SLOTS * 128), BF),
        in_specs=[scalar] + vmem(5),
        name="expert",
    )(place, hidden, *[d.reshape(512, 128) for d in down_parts])
    back = lax.all_to_all(result, "fs", 0, 0, tiled=True)

    pair = jax.ShapeDtypeStruct((SLOTS, count, fs), BF)
    high, low = pl.pallas_call(share_kernel, out_shape=(pair, pair), name="share")(routes, route_weight)
    mixed = pl.pallas_call(
        mix_kernel, out_shape=jax.ShapeDtypeStruct((count, 512), BF), name="mix"
    )(high, low, back)
    down_out = pl.pallas_call(
        down_kernel, out_shape=jax.ShapeDtypeStruct((128, fs * 16), BF), name="down"
    )(got)
    both = both.reshape(1, fs * 16, 256)
    return (both[:, :, :128], both[:, :, 128:], down_out[None], mixed)


def solution(mesh):
    in_specs = (
        P("fs", "tp"),
        P("fs", None),
        P("fs", None),
        P("fs"),
        P(None, "fs", "tp"),
        P(None, "fs", "tp"),
        P(None, "tp", "fs"),
    )
    out_specs = (P("fs", None, "tp"), P("fs", None, "tp"), P("fs", "tp", None), P("fs", "tp"))
    return jax.shard_map(local, mesh=mesh, in_specs=in_specs, out_specs=out_specs, check_vma=False)
```

```python
import jax
import jax.numpy as jnp
from jax import lax
from jax.experimental import pallas as pl
from jax.experimental.pallas import tpu as pltpu
from jax.sharding import PartitionSpec as P

SLOTS = 3
BF = jnp.bfloat16
F32 = jnp.float32


LIMIT = pltpu.CompilerParams(vmem_limit_bytes=12 * 2**20)


def vmem(count):
    return [pl.BlockSpec(memory_space=pltpu.VMEM)] * count


def near(value):
    return pltpu.with_memory_space_constraint(value, pltpu.VMEM)


def slot_hits(routes):
    experts = lax.axis_size("fs")
    count = routes.shape[1]
    expert = lax.broadcasted_iota(jnp.int32, (experts, count), 0)
    first = routes[0:1, :] == expert
    second = routes[1:2, :] == expert
    hit = jnp.where(first | second, 1.0, 0.0)
    before = lax.broadcasted_iota(jnp.int32, (count, count), 0) < lax.broadcasted_iota(
        jnp.int32, (count, count), 1
    )
    order = jnp.dot(hit.astype(BF), jnp.where(before, 1.0, 0.0).astype(BF), preferred_element_type=F32)
    return first, hit, order


def pack_kernel(routes_ref, tokens_ref, down_ref, out_ref):
    _, hit, order = slot_hits(routes_ref[...])
    tokens = tokens_ref[...]
    experts = out_ref.shape[0]
    for s in range(SLOTS):
        chosen = jnp.where((hit > 0.0) & (order == float(s)), 1.0, 0.0).astype(BF)
        rows = jnp.dot(chosen, tokens, preferred_element_type=F32)
        out_ref[:, :, s * 128 : (s + 1) * 128] = rows.reshape(experts, 4, 128).astype(BF)
    base = SLOTS * 128
    for k in range(4):
        out_ref[:, :, base + k * 128 : base + (k + 1) * 128] = down_ref[:, 4 * k : 4 * k + 4, :].astype(BF)


def unpack_kernel(place_ref, got_ref, rows_ref, *down_refs):
    sources = got_ref.shape[0]
    for s in range(SLOTS):
        block = got_ref[:, :, s * 128 : (s + 1) * 128].astype(F32)
        rows_ref[s * sources : (s + 1) * sources, :] = block.reshape(sources, 512).astype(BF)
    base = SLOTS * 128
    part = sources // 4
    for shift, ref in enumerate(down_refs):
        start = ((place_ref[0] + shift) % 4) * part
        for k in range(4):
            ref[:, 4 * k : 4 * k + 4, :] = got_ref[
                pl.ds(start, part), :, base + k * 128 : base + (k + 1) * 128
            ]


def down_kernel(got_ref, out_ref):
    sources = got_ref.shape[0]
    base = SLOTS * 128
    parts = [got_ref[:, :, base + k * 128 : base + (k + 1) * 128] for k in range(4)]
    block = jnp.concatenate([p.astype(F32) for p in parts], axis=1)
    out_ref[...] = block.reshape(sources * 16, 128).T.astype(BF)


def scale_kernel(own, left, right, far_low, far_high, out_ref):
    def squares(ref):
        value = ref[...].astype(F32)
        return jnp.sum(value * value, axis=1, keepdims=True)

    far = jnp.concatenate((squares(far_low), squares(far_high)), axis=0)
    total = squares(own) + squares(left) + squares(right) + far
    out_ref[...] = jnp.broadcast_to(lax.rsqrt(total / 2048.0 + 1e-06), out_ref.shape)


def hidden_kernel(place_ref, own, left, right, far_low, far_high, scale_ref, weight_ref, out_ref):
    place = place_ref[0]
    half = far_low.shape[0]

    def product(value, shift):
        return jnp.dot(value, weight_ref[(place + shift) % 4], preferred_element_type=F32)

    for start, far in ((0, far_low), (half, far_high)):
        rows = pl.ds(start, half)
        acc = product(own[rows, :], 0) + product(left[rows, :], 3)
        acc = acc + product(right[rows, :], 1) + product(far[...], 2)
        scale = scale_ref[rows, :]
        gate = acc[:, :128] * scale
        up = acc[:, 128:] * scale
        out_ref[rows, :] = (gate / (1.0 + jnp.exp(-gate)) * up).astype(BF)


def expert_kernel(place_ref, hidden_ref, d0, d1, d2, d3, out_ref):
    acc = None
    for k, ref in enumerate((d0, d1, d2, d3)):
        block = (place_ref[0] + 4 - k) % 4
        part = lax.dot_general(
            hidden_ref[block], ref[...], (((1,), (1,)), ((), ())), preferred_element_type=F32
        )
        acc = part if acc is None else acc + part
    sources = out_ref.shape[0]
    for s in range(SLOTS):
        rows = acc[s * sources : (s + 1) * sources, :].astype(BF).astype(F32)
        out_ref[:, :, s * 128 : (s + 1) * 128] = rows.reshape(sources, 4, 128).astype(BF)


def share_kernel(routes_ref, weight_ref, high_ref, low_ref):
    first, hit, order = slot_hits(routes_ref[...])
    weight = weight_ref[...]
    share = weight / jnp.sum(weight, axis=0, keepdims=True)
    mine = jnp.where(first, share[0:1, :], share[1:2, :])
    for s in range(SLOTS):
        part = jnp.where((hit > 0.0) & (order == float(s)), mine, 0.0).T
        high = part.astype(BF)
        high_ref[s] = high
        low_ref[s] = (part - high.astype(F32)).astype(BF)


def mix_kernel(high_ref, low_ref, back_ref, out_ref):
    experts = back_ref.shape[0]
    acc = None
    for s in range(SLOTS):
        rows = back_ref[:, :, s * 128 : (s + 1) * 128].astype(F32).reshape(experts, 512).astype(BF)
        part = jnp.dot(high_ref[s], rows, preferred_element_type=F32)
        part = part + jnp.dot(low_ref[s], rows, preferred_element_type=F32)
        acc = part if acc is None else acc + part
    out_ref[...] = acc.astype(BF)


def local(tokens, routes, route_weight, gain, gate_weight, up_weight, down_weight):
    place = lax.axis_index("tp").astype(jnp.int32).reshape(1)
    fs = lax.axis_size("fs")
    count = tokens.shape[0]
    wide = SLOTS * 128 + 512
    scalar = pl.BlockSpec(memory_space=pltpu.SMEM)
    routes = routes.T
    route_weight = route_weight.T

    packed = pl.pallas_call(
        pack_kernel, out_shape=jax.ShapeDtypeStruct((fs, 4, wide), BF), name="pack", compiler_params=LIMIT
    )(routes, tokens, jnp.transpose(down_weight, (0, 2, 1)))
    got = lax.all_to_all(packed, "fs", 0, 0, tiled=True)

    gain_rows = gain[None, :, None]
    gate_new = (gain_rows * gate_weight).astype(BF)
    up_new = (gain_rows * up_weight).astype(BF)
    both = lax.all_to_all(jnp.concatenate((gate_new, up_new), axis=2), "fs", 0, 0, tiled=True)

    got = near(got)
    part = pltpu.VMEM((fs // 4, 16, 128), BF)
    rows, *downs = pl.pallas_call(
        unpack_kernel,
        out_shape=(pltpu.VMEM((SLOTS * fs, 512), BF), part, part, part, part),
        in_specs=[scalar] + vmem(1),
        out_specs=tuple(vmem(5)),
        name="unpack", compiler_params=LIMIT,
    )(place, got)

    def shifted(value, k):
        return lax.ppermute(value, "tp", [(i, (i + k) % 4) for i in range(4)])

    half = SLOTS * fs // 2
    left = shifted(rows, 1)
    right = shifted(rows, 3)
    far_high = shifted(left[half:], 1)
    far_low = shifted(right[:half], 3)
    left, right, far_low, far_high, downs = lax.optimization_barrier(
        (left, right, far_low, far_high, downs)
    )
    features = [near(v) for v in (rows, left, right, far_low, far_high)]
    down_parts = [downs[0]] + [shifted(downs[k], k) for k in (1, 2, 3)]
    scale = pl.pallas_call(
        scale_kernel,
        out_shape=pltpu.VMEM((SLOTS * fs, 128), F32),
        in_specs=vmem(5),
        out_specs=vmem(1)[0],
        name="scale", compiler_params=LIMIT,
    )(*features)

    hidden = pl.pallas_call(
        hidden_kernel,
        out_shape=pltpu.VMEM((SLOTS * fs, 128), BF),
        in_specs=[scalar] + vmem(7),
        out_specs=vmem(1)[0],
        name="hidden", compiler_params=LIMIT,
    )(place, *features, scale, near(both.reshape(4, 512, 256)))
    hidden = lax.all_gather(hidden, "tp", axis=0, tiled=False)
    result = pl.pallas_call(
        expert_kernel,
        out_shape=jax.ShapeDtypeStruct((fs, 4, SLOTS * 128), BF),
        in_specs=[scalar] + vmem(5),
        name="expert", compiler_params=LIMIT,
    )(place, near(hidden), *[near(d.reshape(512, 128)) for d in down_parts])
    back = lax.all_to_all(result, "fs", 0, 0, tiled=True)

    pair = pltpu.VMEM((SLOTS, count, fs), BF)
    high, low = pl.pallas_call(
        share_kernel, out_shape=(pair, pair), out_specs=tuple(vmem(2)), name="share", compiler_params=LIMIT
    )(routes, route_weight)
    mixed = pl.pallas_call(
        mix_kernel,
        out_shape=jax.ShapeDtypeStruct((count, 512), BF),
        in_specs=vmem(3),
        name="mix", compiler_params=LIMIT,
    )(near(high), near(low), near(back))
    down_out = pl.pallas_call(
        down_kernel,
        out_shape=jax.ShapeDtypeStruct((128, fs * 16), BF),
        in_specs=vmem(1),
        name="down", compiler_params=LIMIT,
    )(got)
    both = both.reshape(1, fs * 16, 256)
    return (both[:, :, :128], both[:, :, 128:], down_out[None], mixed)


def solution(mesh):
    in_specs = (
        P("fs", "tp"),
        P("fs", None),
        P("fs", None),
        P("fs"),
        P(None, "fs", "tp"),
        P(None, "fs", "tp"),
        P(None, "tp", "fs"),
    )
    out_specs = (P("fs", None, "tp"), P("fs", None, "tp"), P("fs", "tp", None), P("fs", "tp"))
    return jax.shard_map(local, mesh=mesh, in_specs=in_specs, out_specs=out_specs, check_vma=False)
```

```python
import jax
import jax.numpy as jnp
from jax import lax
from jax.experimental import pallas as pl
from jax.experimental.pallas import tpu as pltpu
from jax.sharding import PartitionSpec as P

SLOTS = 3
BF = jnp.bfloat16
F32 = jnp.float32


LIMIT = pltpu.CompilerParams(vmem_limit_bytes=12 * 2**20)


def vmem(count):
    return [pl.BlockSpec(memory_space=pltpu.VMEM)] * count


def near(value):
    return pltpu.with_memory_space_constraint(value, pltpu.VMEM)


def far(value):
    return pltpu.with_memory_space_constraint(value, pltpu.HBM)


def slot_hits(routes):
    experts = lax.axis_size("fs")
    count = routes.shape[1]
    expert = lax.broadcasted_iota(jnp.int32, (experts, count), 0)
    first = routes[0:1, :] == expert
    second = routes[1:2, :] == expert
    hit = jnp.where(first | second, 1.0, 0.0)
    before = lax.broadcasted_iota(jnp.int32, (count, count), 0) < lax.broadcasted_iota(
        jnp.int32, (count, count), 1
    )
    order = jnp.dot(hit.astype(BF), jnp.where(before, 1.0, 0.0).astype(BF), preferred_element_type=F32)
    return first, hit, order


def pack_kernel(routes_ref, tokens_hbm, down_hbm, out_ref, tokens_ref, down_ref, sems):
    parts = sems.shape[0] - 1
    tokens_copy = pltpu.make_async_copy(tokens_hbm, tokens_ref, sems.at[parts])
    tokens_copy.start()
    step = down_ref.shape[0] // parts
    copies = []
    for p in range(parts):
        piece = pl.ds(p * step, step)
        copies.append(pltpu.make_async_copy(down_hbm.at[piece], down_ref.at[piece], sems.at[p]))
        copies[-1].start()
    _, hit, order = slot_hits(routes_ref[...])
    tokens_copy.wait()
    tokens = tokens_ref[...]
    experts = out_ref.shape[0]
    for s in range(SLOTS):
        chosen = jnp.where((hit > 0.0) & (order == float(s)), 1.0, 0.0).astype(BF)
        rows = jnp.dot(chosen, tokens, preferred_element_type=F32)
        out_ref[:, :, s * 128 : (s + 1) * 128] = rows.reshape(experts, 4, 128).astype(BF)
    base = SLOTS * 128
    for p in range(parts):
        copies[p].wait()
        piece = pl.ds(p * step, step)
        for k in range(4):
            out_ref[piece, :, base + k * 128 : base + (k + 1) * 128] = down_ref[
                piece, 4 * k : 4 * k + 4, :
            ].astype(BF)


def unpack_kernel(got_ref, low_ref, high_ref, down_ref):
    sources = got_ref.shape[0]
    half = low_ref.shape[0]
    blocks = []
    for s in range(SLOTS):
        block = got_ref[:, :, s * 128 : (s + 1) * 128].astype(F32)
        blocks.append(block.reshape(sources, 512).astype(BF))
    low_ref[:sources, :] = blocks[0]
    low_ref[sources:, :] = blocks[1][: half - sources, :]
    high_ref[: 2 * sources - half, :] = blocks[1][half - sources :, :]
    high_ref[2 * sources - half :, :] = blocks[2]
    base = SLOTS * 128
    for k in range(4):
        down_ref[:, 4 * k : 4 * k + 4, :] = got_ref[:, :, base + k * 128 : base + (k + 1) * 128]


def down_kernel(down_ref, out_ref):
    out_ref[...] = down_ref[...].astype(F32).T.astype(BF)


def scale_kernel(low_ref, high_ref, out_ref):
    half = low_ref.shape[1]
    for h, ref in enumerate((low_ref, high_ref)):
        total = None
        for k in range(4):
            value = ref[k].astype(F32)
            part = jnp.sum(value * value, axis=1, keepdims=True)
            total = part if total is None else total + part
        scale = lax.rsqrt(total / 2048.0 + 1e-06)
        out_ref[h * half : (h + 1) * half, :] = jnp.broadcast_to(scale, (half, 128))


def hidden_kernel(low_ref, high_ref, scale_ref, weight_ref, down_ref, out_ref):
    half = low_ref.shape[1]
    total = 2 * half
    for h, ref in enumerate((low_ref, high_ref)):
        acc = None
        for k in range(4):
            part = jnp.dot(ref[k], weight_ref[k], preferred_element_type=F32)
            acc = part if acc is None else acc + part
        scale = scale_ref[h * half : (h + 1) * half, :]
        gate = acc[:, :128] * scale
        up = acc[:, 128:] * scale
        hidden = (gate / (1.0 + jnp.exp(-gate)) * up).astype(BF)
        for k in range(4):
            out_ref[k, h * half : (h + 1) * half, :] = hidden
    for k in range(4):
        out_ref[k, total:, :] = down_ref[k]


def expert_kernel(got_ref, out_ref):
    sources = out_ref.shape[0]
    total = SLOTS * sources
    acc = None
    for k in range(4):
        part = lax.dot_general(
            got_ref[k, :total, :],
            got_ref[k, total:, :],
            (((1,), (1,)), ((), ())),
            preferred_element_type=F32,
        )
        acc = part if acc is None else acc + part
    for s in range(SLOTS):
        rows = acc[s * sources : (s + 1) * sources, :].astype(BF).astype(F32)
        out_ref[:, :, s * 128 : (s + 1) * 128] = rows.reshape(sources, 4, 128).astype(BF)


def share_kernel(routes_ref, weight_ref, high_ref, low_ref):
    first, hit, order = slot_hits(routes_ref[...])
    weight = weight_ref[...]
    share = weight / jnp.sum(weight, axis=0, keepdims=True)
    mine = jnp.where(first, share[0:1, :], share[1:2, :])
    for s in range(SLOTS):
        part = jnp.where((hit > 0.0) & (order == float(s)), mine, 0.0).T
        high = part.astype(BF)
        high_ref[s] = high
        low_ref[s] = (part - high.astype(F32)).astype(BF)


def mix_kernel(high_ref, low_ref, back_ref, out_ref):
    experts = back_ref.shape[0]
    acc = None
    for s in range(SLOTS):
        rows = back_ref[:, :, s * 128 : (s + 1) * 128].astype(F32).reshape(experts, 512).astype(BF)
        part = jnp.dot(high_ref[s], rows, preferred_element_type=F32)
        part = part + jnp.dot(low_ref[s], rows, preferred_element_type=F32)
        acc = part if acc is None else acc + part
    out_ref[...] = acc.astype(BF)


def call(kernel, name, outs, in_specs, args, scratch=()):
    many = isinstance(outs, tuple)
    return pl.pallas_call(
        kernel,
        out_shape=outs,
        in_specs=in_specs,
        out_specs=tuple(vmem(len(outs))) if many else vmem(1)[0],
        scratch_shapes=scratch,
        compiler_params=LIMIT,
        name=name,
    )(*args)


def local(tokens, routes, route_weight, gain, gate_weight, up_weight, down_weight):
    fs = lax.axis_size("fs")
    count = tokens.shape[0]
    rows = SLOTS * fs
    wide = SLOTS * 128 + 512
    hbm = pl.BlockSpec(memory_space=pltpu.HBM)
    plain = jax.ShapeDtypeStruct
    routes = routes.T
    route_weight = route_weight.T

    packed = call(
        pack_kernel,
        "pack",
        plain((fs, 4, wide), BF),
        vmem(1) + [hbm, hbm],
        (far(routes), far(tokens), far(jnp.transpose(down_weight, (0, 2, 1)))),
        [
            pltpu.VMEM((count, 512), BF),
            pltpu.VMEM((fs, 16, 128), F32),
            pltpu.SemaphoreType.DMA((5,)),
        ],
    )
    got = near(lax.all_to_all(packed, "fs", 0, 0, tiled=True))

    gain_rows = gain[None, :, None]
    gate_new = (gain_rows * gate_weight).astype(BF)
    up_new = (gain_rows * up_weight).astype(BF)
    both = lax.all_to_all(jnp.concatenate((gate_new, up_new), axis=2), "fs", 0, 0, tiled=True)

    part = pltpu.VMEM((rows // 2, 512), BF)
    low, high, down = call(
        unpack_kernel, "unpack", (part, part, plain((fs, 16, 128), BF)), vmem(1), (got,)
    )
    low = lax.all_gather(low, "tp", axis=0, tiled=False)
    low, high = lax.optimization_barrier((low, high))
    high = lax.all_gather(high, "tp", axis=0, tiled=False)
    low, high = near(low), near(high)
    scale = call(scale_kernel, "scale", pltpu.VMEM((rows, 128), F32), vmem(2), (low, high))
    payload = call(
        hidden_kernel,
        "hidden",
        plain((4, rows + 512, 128), BF),
        vmem(5),
        (low, high, scale, near(both.reshape(4, 512, 256)), down.reshape(4, 512, 128)),
    )
    payload = near(lax.all_to_all(payload, "tp", 0, 0, tiled=True))
    result = call(expert_kernel, "expert", plain((fs, 4, SLOTS * 128), BF), vmem(1), (payload,))
    back = near(lax.all_to_all(result, "fs", 0, 0, tiled=True))

    pair = pltpu.VMEM((SLOTS, count, fs), BF)
    shares = call(share_kernel, "share", (pair, pair), vmem(2), (routes, route_weight))
    mixed = call(mix_kernel, "mix", plain((count, 512), BF), vmem(3), (*shares, back))
    down_out = call(
        down_kernel, "down", plain((128, fs * 16), BF), vmem(1), (down.reshape(fs * 16, 128),)
    )
    both = both.reshape(1, fs * 16, 256)
    return (both[:, :, :128], both[:, :, 128:], down_out[None], mixed)


def solution(mesh):
    in_specs = (
        P("fs", "tp"),
        P("fs", None),
        P("fs", None),
        P("fs"),
        P(None, "fs", "tp"),
        P(None, "fs", "tp"),
        P(None, "tp", "fs"),
    )
    out_specs = (P("fs", None, "tp"), P("fs", None, "tp"), P("fs", "tp", None), P("fs", "tp"))
    return jax.shard_map(local, mesh=mesh, in_specs=in_specs, out_specs=out_specs, check_vma=False)
```

```python
import jax
import jax.numpy as jnp
from jax import lax
from jax.experimental import pallas as pl
from jax.experimental.pallas import tpu as pltpu
from jax.sharding import PartitionSpec as P

SLOTS = 3
BF = jnp.bfloat16
F32 = jnp.float32


LIMIT = pltpu.CompilerParams(vmem_limit_bytes=12 * 2**20)


def vmem(count):
    return [pl.BlockSpec(memory_space=pltpu.VMEM)] * count


def near(value):
    return pltpu.with_memory_space_constraint(value, pltpu.VMEM)


def far(value):
    return pltpu.with_memory_space_constraint(value, pltpu.HBM)


def slot_hits(routes):
    experts = lax.axis_size("fs")
    count = routes.shape[1]
    expert = lax.broadcasted_iota(jnp.int32, (experts, count), 0)
    first = routes[0:1, :] == expert
    second = routes[1:2, :] == expert
    hit = jnp.where(first | second, 1.0, 0.0)
    before = lax.broadcasted_iota(jnp.int32, (count, count), 0) < lax.broadcasted_iota(
        jnp.int32, (count, count), 1
    )
    order = jnp.dot(hit.astype(BF), jnp.where(before, 1.0, 0.0).astype(BF), preferred_element_type=F32)
    return first, hit, order


def pack_kernel(routes_ref, tokens_ref, out_ref):
    _, hit, order = slot_hits(routes_ref[...])
    tokens = tokens_ref[...]
    experts = out_ref.shape[0]
    for s in range(SLOTS):
        chosen = jnp.where((hit > 0.0) & (order == float(s)), 1.0, 0.0).astype(BF)
        rows = jnp.dot(chosen, tokens, preferred_element_type=F32)
        out_ref[:, :, s * 128 : (s + 1) * 128] = rows.reshape(experts, 4, 128).astype(BF)


def unpack_kernel(got_ref, low_ref, high_ref):
    sources = got_ref.shape[0]
    half = low_ref.shape[0]
    blocks = []
    for s in range(SLOTS):
        block = got_ref[:, :, s * 128 : (s + 1) * 128].astype(F32)
        blocks.append(block.reshape(sources, 512).astype(BF))
    low_ref[:sources, :] = blocks[0]
    low_ref[sources:, :] = blocks[1][: half - sources, :]
    high_ref[: 2 * sources - half, :] = blocks[1][half - sources :, :]
    high_ref[2 * sources - half :, :] = blocks[2]


def place_kernel(weight_ref, gate_ref, up_ref, down_ref):
    gate_ref[...] = weight_ref[:, :16, :]
    up_ref[...] = weight_ref[:, 16:32, :]
    block = weight_ref[:, 32:, :].reshape(weight_ref.shape[0] * 16, 128)
    down_ref[...] = block.astype(F32).T.astype(BF)


def scale_kernel(low_ref, high_ref, out_ref):
    half = low_ref.shape[1]
    for h, ref in enumerate((low_ref, high_ref)):
        total = None
        for k in range(4):
            value = ref[k].astype(F32)
            part = jnp.sum(value * value, axis=1, keepdims=True)
            total = part if total is None else total + part
        scale = lax.rsqrt(total / 2048.0 + 1e-06)
        out_ref[h * half : (h + 1) * half, :] = jnp.broadcast_to(scale, (half, 128))


def hidden_kernel(low_ref, high_ref, scale_ref, weight_ref, out_ref):
    half = low_ref.shape[1]
    total = 2 * half
    part = weight_ref.shape[0] // 4

    def block(k, kind):
        piece = weight_ref[k * part : (k + 1) * part, 16 * kind : 16 * kind + 16, :]
        return piece.reshape(part * 16, 128)

    accs = [None, None]
    for k in range(4):
        weight = jnp.concatenate((block(k, 0), block(k, 1)), axis=1)
        for h, ref in enumerate((low_ref, high_ref)):
            product = jnp.dot(ref[k], weight, preferred_element_type=F32)
            accs[h] = product if k == 0 else accs[h] + product
        out_ref[k, total:, :] = block(k, 2)
    for h in range(2):
        scale = scale_ref[h * half : (h + 1) * half, :]
        gate = accs[h][:, :128] * scale
        up = accs[h][:, 128:] * scale
        hidden = (gate / (1.0 + jnp.exp(-gate)) * up).astype(BF)
        for k in range(4):
            out_ref[k, h * half : (h + 1) * half, :] = hidden


def expert_kernel(got_ref, out_ref):
    sources = out_ref.shape[0]
    total = SLOTS * sources
    acc = None
    for k in range(4):
        part = lax.dot_general(
            got_ref[k, :total, :],
            got_ref[k, total:, :],
            (((1,), (1,)), ((), ())),
            preferred_element_type=F32,
        )
        acc = part if acc is None else acc + part
    for s in range(SLOTS):
        rows = acc[s * sources : (s + 1) * sources, :].astype(BF).astype(F32)
        out_ref[:, :, s * 128 : (s + 1) * 128] = rows.reshape(sources, 4, 128).astype(BF)


def share_kernel(routes_ref, weight_ref, high_ref, low_ref):
    first, hit, order = slot_hits(routes_ref[...])
    weight = weight_ref[...]
    share = weight / jnp.sum(weight, axis=0, keepdims=True)
    mine = jnp.where(first, share[0:1, :], share[1:2, :])
    for s in range(SLOTS):
        part = jnp.where((hit > 0.0) & (order == float(s)), mine, 0.0).T
        high = part.astype(BF)
        high_ref[s] = high
        low_ref[s] = (part - high.astype(F32)).astype(BF)


def mix_kernel(high_ref, low_ref, back_ref, out_ref):
    experts = back_ref.shape[0]
    acc = None
    for s in range(SLOTS):
        rows = back_ref[:, :, s * 128 : (s + 1) * 128].astype(F32).reshape(experts, 512).astype(BF)
        part = jnp.dot(high_ref[s], rows, preferred_element_type=F32)
        part = part + jnp.dot(low_ref[s], rows, preferred_element_type=F32)
        acc = part if acc is None else acc + part
    out_ref[...] = acc.astype(BF)


def call(kernel, name, outs, in_specs, args, scratch=()):
    many = isinstance(outs, tuple)
    return pl.pallas_call(
        kernel,
        out_shape=outs,
        in_specs=in_specs,
        out_specs=tuple(vmem(len(outs))) if many else vmem(1)[0],
        scratch_shapes=scratch,
        compiler_params=LIMIT,
        name=name,
    )(*args)


def local(tokens, routes, route_weight, gain, gate_weight, up_weight, down_weight):
    fs = lax.axis_size("fs")
    count = tokens.shape[0]
    rows = SLOTS * fs
    plain = jax.ShapeDtypeStruct
    routes = routes.T
    route_weight = route_weight.T

    packed = call(
        pack_kernel, "pack", plain((fs, 4, SLOTS * 128), BF), vmem(2), (far(routes), far(tokens))
    )
    got = near(lax.all_to_all(packed, "fs", 0, 0, tiled=True))

    gain_rows = gain[None, :, None]
    parts = (gain_rows * gate_weight, gain_rows * up_weight, jnp.transpose(down_weight, (0, 2, 1)))
    weights = jnp.concatenate([p.astype(BF) for p in parts], axis=1)
    weights = near(lax.all_to_all(weights, "fs", 0, 0, tiled=True))

    part = pltpu.VMEM((rows // 2, 512), BF)
    low, high = call(unpack_kernel, "unpack", (part, part), vmem(1), (got,))
    low = lax.all_gather(low, "tp", axis=0, tiled=False)
    low, high = lax.optimization_barrier((low, high))
    high = lax.all_gather(high, "tp", axis=0, tiled=False)
    low, high = near(low), near(high)
    scale = call(scale_kernel, "scale", pltpu.VMEM((rows, 128), F32), vmem(2), (low, high))
    payload = call(
        hidden_kernel,
        "hidden",
        plain((4, rows + 512, 128), BF),
        vmem(4),
        (low, high, scale, weights),
    )
    payload = near(lax.all_to_all(payload, "tp", 0, 0, tiled=True))
    result = call(expert_kernel, "expert", plain((fs, 4, SLOTS * 128), BF), vmem(1), (payload,))
    back = near(lax.all_to_all(result, "fs", 0, 0, tiled=True))

    pair = pltpu.VMEM((SLOTS, count, fs), BF)
    shares = call(share_kernel, "share", (pair, pair), vmem(2), (routes, route_weight))
    mixed = call(mix_kernel, "mix", plain((count, 512), BF), vmem(3), (*shares, back))
    part = plain((fs, 16, 128), BF)
    gate_out, up_out, down_out = call(
        place_kernel, "place", (part, part, plain((128, fs * 16), BF)), vmem(1), (weights,)
    )
    wide = (1, fs * 16, 128)
    return (gate_out.reshape(wide), up_out.reshape(wide), down_out[None], mixed)


def solution(mesh):
    in_specs = (
        P("fs", "tp"),
        P("fs", None),
        P("fs", None),
        P("fs"),
        P(None, "fs", "tp"),
        P(None, "fs", "tp"),
        P(None, "tp", "fs"),
    )
    out_specs = (P("fs", None, "tp"), P("fs", None, "tp"), P("fs", "tp", None), P("fs", "tp"))
    return jax.shard_map(local, mesh=mesh, in_specs=in_specs, out_specs=out_specs, check_vma=False)
```

```python
import jax
import jax.numpy as jnp
from jax import lax
from jax.experimental import pallas as pl
from jax.experimental.pallas import tpu as pltpu
from jax.sharding import PartitionSpec as P

SLOTS = 3
BF = jnp.bfloat16
F32 = jnp.float32


LIMIT = pltpu.CompilerParams(vmem_limit_bytes=12 * 2**20)


def vmem(count):
    return [pl.BlockSpec(memory_space=pltpu.VMEM)] * count


def near(value):
    return pltpu.with_memory_space_constraint(value, pltpu.VMEM)


def far(value):
    return pltpu.with_memory_space_constraint(value, pltpu.HBM)


def slot_hits(routes):
    experts = lax.axis_size("fs")
    count = routes.shape[1]
    expert = lax.broadcasted_iota(jnp.int32, (experts, count), 0)
    first = routes[0:1, :] == expert
    second = routes[1:2, :] == expert
    hit = jnp.where(first | second, 1.0, 0.0)
    before = lax.broadcasted_iota(jnp.int32, (count, count), 0) < lax.broadcasted_iota(
        jnp.int32, (count, count), 1
    )
    order = jnp.dot(hit.astype(BF), jnp.where(before, 1.0, 0.0).astype(BF), preferred_element_type=F32)
    return first, hit, order


def pack_kernel(routes_ref, tokens_hbm, down_hbm, out_ref, tokens_ref, down_ref, sems):
    parts = sems.shape[0] - 1
    tokens_copy = pltpu.make_async_copy(tokens_hbm, tokens_ref, sems.at[parts])
    tokens_copy.start()
    step = down_ref.shape[0] // parts
    copies = []
    for p in range(parts):
        piece = pl.ds(p * step, step)
        copies.append(pltpu.make_async_copy(down_hbm.at[piece], down_ref.at[piece], sems.at[p]))
        copies[-1].start()
    _, hit, order = slot_hits(routes_ref[...])
    tokens_copy.wait()
    tokens = tokens_ref[...]
    experts = out_ref.shape[0]
    for s in range(SLOTS):
        chosen = jnp.where((hit > 0.0) & (order == float(s)), 1.0, 0.0).astype(BF)
        rows = jnp.dot(chosen, tokens, preferred_element_type=F32)
        out_ref[:, :, s * 128 : (s + 1) * 128] = rows.reshape(experts, 4, 128).astype(BF)
    base = SLOTS * 128
    for p in range(parts):
        copies[p].wait()
        piece = pl.ds(p * step, step)
        for k in range(4):
            out_ref[piece, :, base + k * 128 : base + (k + 1) * 128] = down_ref[
                piece, 4 * k : 4 * k + 4, :
            ].astype(BF)


def unpack_kernel(place_ref, got_ref, down_ref, main_ref, *piece_refs):
    sources = got_ref.shape[0]
    main = main_ref.shape[0]
    blocks = []
    for s in range(SLOTS):
        block = got_ref[:, :, s * 128 : (s + 1) * 128].astype(F32)
        blocks.append(block.reshape(sources, 512).astype(BF))
    main_ref[:sources, :] = blocks[0]
    main_ref[sources:, :] = blocks[1][: main - sources, :]
    rest = jnp.concatenate((blocks[1][main - sources :, :], blocks[2]), axis=0)
    count = rest.shape[0]
    part = sources // 4
    base = SLOTS * 128
    for k in range(4):
        down_ref[:, 4 * k : 4 * k + 4, :] = got_ref[:, :, base + k * 128 : base + (k + 1) * 128]
    for shift, ref in enumerate(piece_refs):
        for c in range(4):
            ref[c * count : (c + 1) * count, :] = rest[:, c * 128 : (c + 1) * 128]
        start = ((place_ref[0] + shift) % 4) * part
        ref[4 * count :, :] = down_ref[pl.ds(start, part), :, :].reshape(part * 16, 128)


def other_rows(ref):
    count = (ref.shape[0] - 512) // 4
    return jnp.concatenate([ref[c * count : (c + 1) * count, :] for c in range(4)], axis=1)


def scale_kernel(main_ref, p0, p1, p2, p3, out_ref):
    main = main_ref.shape[1]

    def scales(values):
        total = None
        for value in values:
            value = value.astype(F32)
            part = jnp.sum(value * value, axis=1, keepdims=True)
            total = part if total is None else total + part
        scale = lax.rsqrt(total / 2048.0 + 1e-06)
        return jnp.broadcast_to(scale, (scale.shape[0], 128))

    out_ref[:main, :] = scales([main_ref[k] for k in range(4)])
    out_ref[main:, :] = scales([other_rows(ref) for ref in (p0, p1, p2, p3)])


def hidden_kernel(place_ref, main_ref, p0, p1, p2, p3, scale_ref, weight_ref, out_ref):
    main = main_ref.shape[1]
    part = weight_ref.shape[0] // 4

    def product(rows, block):
        weight = weight_ref[pl.ds(block * part, part), :, :].reshape(part * 16, 256)
        return jnp.dot(rows, weight, preferred_element_type=F32)

    def finish(acc, start):
        count = acc.shape[0]
        scale = scale_ref[start : start + count, :]
        gate = acc[:, :128] * scale
        up = acc[:, 128:] * scale
        out_ref[start : start + count, :] = (gate / (1.0 + jnp.exp(-gate)) * up).astype(BF)

    acc = product(main_ref[0], 0)
    for k in range(1, 4):
        acc = acc + product(main_ref[k], k)
    finish(acc, 0)
    acc = product(other_rows(p0), place_ref[0])
    for k, ref in ((1, p1), (2, p2), (3, p3)):
        acc = acc + product(other_rows(ref), (place_ref[0] + 4 - k) % 4)
    finish(acc, main)


def expert_kernel(place_ref, hidden_ref, p0, p1, p2, p3, out_ref):
    sources = out_ref.shape[0]
    hidden = [hidden_ref[(place_ref[0] + 4 - k) % 4] for k in range(4)]
    down = [ref[ref.shape[0] - 512 :, :] for ref in (p0, p1, p2, p3)]
    result = lax.dot_general(
        jnp.concatenate(hidden, axis=1),
        jnp.concatenate(down, axis=1),
        (((1,), (1,)), ((), ())),
        preferred_element_type=F32,
    )
    for s in range(SLOTS):
        rows = result[s * sources : (s + 1) * sources, :]
        out_ref[:, :, s * 128 : (s + 1) * 128] = rows.reshape(sources, 4, 128).astype(BF)


def place_kernel(rows_ref, weight_ref, gate_ref, up_ref, down_ref):
    gate_ref[...] = weight_ref[:, :, :128]
    up_ref[...] = weight_ref[:, :, 128:]
    down_ref[...] = rows_ref[...].astype(F32).T.astype(BF)


def share_kernel(routes_ref, weight_ref, high_ref, low_ref):
    first, hit, order = slot_hits(routes_ref[...])
    weight = weight_ref[...]
    share = weight / jnp.sum(weight, axis=0, keepdims=True)
    mine = jnp.where(first, share[0:1, :], share[1:2, :])
    for s in range(SLOTS):
        part = jnp.where((hit > 0.0) & (order == float(s)), mine, 0.0).T
        high = part.astype(BF)
        high_ref[s] = high
        low_ref[s] = (part - high.astype(F32)).astype(BF)


def mix_kernel(high_ref, low_ref, back_ref, out_ref):
    experts = back_ref.shape[0]
    acc = None
    for s in range(SLOTS):
        rows = back_ref[:, :, s * 128 : (s + 1) * 128].astype(F32).reshape(experts, 512).astype(BF)
        part = jnp.dot(high_ref[s], rows, preferred_element_type=F32)
        part = part + jnp.dot(low_ref[s], rows, preferred_element_type=F32)
        acc = part if acc is None else acc + part
    out_ref[...] = acc.astype(BF)


def call(kernel, name, outs, in_specs, args, scratch=()):
    many = isinstance(outs, tuple)
    return pl.pallas_call(
        kernel,
        out_shape=outs,
        in_specs=in_specs,
        out_specs=tuple(vmem(len(outs))) if many else vmem(1)[0],
        scratch_shapes=scratch,
        compiler_params=LIMIT,
        name=name,
    )(*args)


def local(tokens, routes, route_weight, gain, gate_weight, up_weight, down_weight):
    place = lax.axis_index("tp").astype(jnp.int32).reshape(1)
    fs = lax.axis_size("fs")
    count = tokens.shape[0]
    rows = SLOTS * fs
    main = 240
    scalar = [pl.BlockSpec(memory_space=pltpu.SMEM)]
    hbm = pl.BlockSpec(memory_space=pltpu.HBM)
    plain = jax.ShapeDtypeStruct
    routes = routes.T
    route_weight = route_weight.T

    packed = call(
        pack_kernel,
        "pack",
        plain((fs, 4, SLOTS * 128 + 512), BF),
        vmem(1) + [hbm, hbm],
        (far(routes), far(tokens), far(jnp.transpose(down_weight, (0, 2, 1)))),
        [
            pltpu.VMEM((count, 512), BF),
            pltpu.VMEM((fs, 16, 128), F32),
            pltpu.SemaphoreType.DMA((5,)),
        ],
    )
    got = near(lax.all_to_all(packed, "fs", 0, 0, tiled=True))

    gain_rows = gain[None, :, None]
    weights = [(gain_rows * w).astype(BF) for w in (gate_weight, up_weight)]
    weights = near(lax.all_to_all(jnp.concatenate(weights, axis=2), "fs", 0, 0, tiled=True))

    piece = pltpu.VMEM((4 * (rows - main) + 512, 128), BF)
    part = plain((fs, 16, 128), BF)
    down, gathered, *pieces = call(
        unpack_kernel,
        "unpack",
        (part, pltpu.VMEM((main, 512), BF), piece, piece, piece, piece),
        scalar + vmem(1),
        (place, got),
    )
    own = pieces[0]
    moved = {
        k: near(lax.ppermute(pieces[k], "tp", [(i, (i + k) % 4) for i in range(4)]))
        for k in (1, 3, 2)
    }
    pieces = (own, moved[1], moved[2], moved[3])
    gathered = near(lax.all_gather(gathered, "tp", axis=0, tiled=False))
    scale = call(
        scale_kernel, "scale", pltpu.VMEM((rows, 128), F32), vmem(5), (gathered, *pieces)
    )
    hidden = call(
        hidden_kernel,
        "hidden",
        pltpu.VMEM((rows, 128), BF),
        scalar + vmem(7),
        (place, gathered, *pieces, scale, weights),
    )
    hidden = near(lax.all_gather(hidden, "tp", axis=0, tiled=False))
    result = call(
        expert_kernel,
        "expert",
        plain((fs, 4, SLOTS * 128), BF),
        scalar + vmem(5),
        (place, hidden, *pieces),
    )
    back = near(lax.all_to_all(result, "fs", 0, 0, tiled=True))

    pair = pltpu.VMEM((SLOTS, count, fs), BF)
    shares = call(share_kernel, "share", (pair, pair), vmem(2), (routes, route_weight))
    mixed = call(mix_kernel, "mix", plain((count, 512), BF), vmem(3), (*shares, back))
    gate_out, up_out, down_out = call(
        place_kernel,
        "place",
        (part, part, plain((128, fs * 16), BF)),
        vmem(2),
        (far(down.reshape(fs * 16, 128)), weights),
    )
    wide = (1, fs * 16, 128)
    return (gate_out.reshape(wide), up_out.reshape(wide), down_out[None], mixed)


def solution(mesh):
    in_specs = (
        P("fs", "tp"),
        P("fs", None),
        P("fs", None),
        P("fs"),
        P(None, "fs", "tp"),
        P(None, "fs", "tp"),
        P(None, "tp", "fs"),
    )
    out_specs = (P("fs", None, "tp"), P("fs", None, "tp"), P("fs", "tp", None), P("fs", "tp"))
    return jax.shard_map(local, mesh=mesh, in_specs=in_specs, out_specs=out_specs, check_vma=False)
```

```python
import jax
import jax.numpy as jnp
from jax import lax
from jax.experimental import pallas as pl
from jax.experimental.pallas import tpu as pltpu
from jax.sharding import PartitionSpec as P

SLOTS = 3
BF = jnp.bfloat16
F32 = jnp.float32


LIMIT = pltpu.CompilerParams(vmem_limit_bytes=12 * 2**20)


def vmem(count):
    return [pl.BlockSpec(memory_space=pltpu.VMEM)] * count


def near(value):
    return pltpu.with_memory_space_constraint(value, pltpu.VMEM)


def far(value):
    return pltpu.with_memory_space_constraint(value, pltpu.HBM)


def slot_hits(routes):
    experts = lax.axis_size("fs")
    count = routes.shape[1]
    expert = lax.broadcasted_iota(jnp.int32, (experts, count), 0)
    first = routes[0:1, :] == expert
    second = routes[1:2, :] == expert
    hit = jnp.where(first | second, 1.0, 0.0)
    before = lax.broadcasted_iota(jnp.int32, (count, count), 0) < lax.broadcasted_iota(
        jnp.int32, (count, count), 1
    )
    order = jnp.dot(hit.astype(BF), jnp.where(before, 1.0, 0.0).astype(BF), preferred_element_type=F32)
    return first, hit, order


def pack_kernel(routes_ref, tokens_ref, out_ref, rows_ref, sems):
    _, hit, order = slot_hits(routes_ref[...])
    tokens = tokens_ref[...]
    step = rows_ref.shape[0] // 2
    chosen = [jnp.where((hit > 0.0) & (order == float(s)), 1.0, 0.0).astype(BF) for s in range(SLOTS)]
    copies = []
    for h in range(2):
        piece = slice(h * step, (h + 1) * step)
        rows = jnp.dot(
            jnp.concatenate([c[piece] for c in chosen], axis=0), tokens, preferred_element_type=F32
        )
        for s in range(SLOTS):
            part = rows[s * step : (s + 1) * step].reshape(step, 4, 128)
            rows_ref[piece, :, s * 128 : (s + 1) * 128] = part.astype(BF)
        copies.append(pltpu.make_async_copy(rows_ref.at[piece], out_ref.at[piece], sems.at[h]))
        copies[-1].start()
    for copy in copies:
        copy.wait()


def unpack_kernel(got_ref, low_ref, high_ref):
    sources = got_ref.shape[0]
    half = low_ref.shape[0]
    blocks = []
    for s in range(SLOTS):
        block = got_ref[:, :, s * 128 : (s + 1) * 128].astype(F32)
        blocks.append(block.reshape(sources, 512).astype(BF))
    low_ref[:sources, :] = blocks[0]
    low_ref[sources:, :] = blocks[1][: half - sources, :]
    high_ref[: 2 * sources - half, :] = blocks[1][half - sources :, :]
    high_ref[2 * sources - half :, :] = blocks[2]


def place_kernel(weight_ref, gate_ref, up_ref, down_ref):
    gate_ref[...] = weight_ref[:, :16, :]
    up_ref[...] = weight_ref[:, 16:32, :]
    block = weight_ref[:, 32:, :].reshape(weight_ref.shape[0] * 16, 128)
    down_ref[...] = block.astype(F32).T.astype(BF)


def scale_kernel(low_ref, high_ref, out_ref):
    half = low_ref.shape[1]
    for h, ref in enumerate((low_ref, high_ref)):
        total = None
        for k in range(4):
            value = ref[k].astype(F32)
            part = jnp.sum(value * value, axis=1, keepdims=True)
            total = part if total is None else total + part
        scale = lax.rsqrt(total / 2048.0 + 1e-06)
        out_ref[h * half : (h + 1) * half, :] = jnp.broadcast_to(scale, (half, 128))


def hidden_kernel(low_ref, high_ref, scale_ref, weight_ref, out_ref):
    half = low_ref.shape[1]
    total = 2 * half
    part = weight_ref.shape[0] // 4

    def block(k, kind):
        piece = weight_ref[k * part : (k + 1) * part, 16 * kind : 16 * kind + 16, :]
        return piece.reshape(part * 16, 128)

    accs = [None, None]
    for k in range(4):
        weight = jnp.concatenate((block(k, 0), block(k, 1)), axis=1)
        for h, ref in enumerate((low_ref, high_ref)):
            product = jnp.dot(ref[k], weight, preferred_element_type=F32)
            accs[h] = product if k == 0 else accs[h] + product
        out_ref[k, total:, :] = block(k, 2)
    for h in range(2):
        scale = scale_ref[h * half : (h + 1) * half, :]
        gate = accs[h][:, :128] * scale
        up = accs[h][:, 128:] * scale
        hidden = (gate / (1.0 + jnp.exp(-gate)) * up).astype(BF)
        for k in range(4):
            out_ref[k, h * half : (h + 1) * half, :] = hidden


def expert_kernel(got_ref, out_ref):
    sources = out_ref.shape[0]
    total = SLOTS * sources
    result = lax.dot_general(
        jnp.concatenate([got_ref[k, :total, :] for k in range(4)], axis=1),
        jnp.concatenate([got_ref[k, total:, :] for k in range(4)], axis=1),
        (((1,), (1,)), ((), ())),
        preferred_element_type=F32,
    )
    for s in range(SLOTS):
        rows = result[s * sources : (s + 1) * sources, :]
        out_ref[:, :, s * 128 : (s + 1) * 128] = rows.reshape(sources, 4, 128).astype(BF)


def share_kernel(routes_ref, weight_ref, out_ref):
    first, hit, order = slot_hits(routes_ref[...])
    weight = weight_ref[...]
    share = weight / jnp.sum(weight, axis=0, keepdims=True)
    mine = jnp.where(first, share[0:1, :], share[1:2, :])
    count = out_ref.shape[0] // 2
    for s in range(SLOTS):
        part = jnp.where((hit > 0.0) & (order == float(s)), mine, 0.0).T
        high = part.astype(BF)
        columns = slice(s * part.shape[1], (s + 1) * part.shape[1])
        out_ref[:count, columns] = high
        out_ref[count:, columns] = (part - high.astype(F32)).astype(BF)


def mix_kernel(share_ref, back_ref, out_ref):
    experts = back_ref.shape[0]
    blocks = []
    for s in range(SLOTS):
        block = back_ref[:, :, s * 128 : (s + 1) * 128].astype(F32)
        blocks.append(block.reshape(experts, 512).astype(BF))
    both = jnp.dot(share_ref[...], jnp.concatenate(blocks, axis=0), preferred_element_type=F32)
    count = out_ref.shape[0]
    out_ref[...] = (both[:count] + both[count:]).astype(BF)


def call(kernel, name, outs, in_specs, args, scratch=()):
    many = isinstance(outs, tuple)
    return pl.pallas_call(
        kernel,
        out_shape=outs,
        in_specs=in_specs,
        out_specs=tuple(vmem(len(outs))) if many else vmem(1)[0],
        scratch_shapes=scratch,
        compiler_params=LIMIT,
        name=name,
    )(*args)


def local(tokens, routes, route_weight, gain, gate_weight, up_weight, down_weight):
    fs = lax.axis_size("fs")
    count = tokens.shape[0]
    rows = SLOTS * fs
    plain = jax.ShapeDtypeStruct
    routes = routes.T
    route_weight = route_weight.T

    slots = (fs, 4, SLOTS * 128)
    packed = pl.pallas_call(
        pack_kernel,
        out_shape=plain(slots, BF),
        in_specs=vmem(2),
        out_specs=pl.BlockSpec(memory_space=pltpu.HBM),
        scratch_shapes=[pltpu.VMEM(slots, BF), pltpu.SemaphoreType.DMA((2,))],
        compiler_params=LIMIT,
        name="pack",
    )(far(routes), far(tokens))
    got = near(lax.all_to_all(packed, "fs", 0, 0, tiled=True))

    gain_rows = gain[None, :, None]
    parts = (gain_rows * gate_weight, gain_rows * up_weight, jnp.transpose(down_weight, (0, 2, 1)))
    weights = jnp.concatenate([p.astype(BF) for p in parts], axis=1)
    weights = near(lax.all_to_all(weights, "fs", 0, 0, tiled=True))

    part = pltpu.VMEM((rows // 2, 512), BF)
    low, high = call(unpack_kernel, "unpack", (part, part), vmem(1), (got,))
    low = lax.all_gather(low, "tp", axis=0, tiled=False)
    low, high = lax.optimization_barrier((low, high))
    high = lax.all_gather(high, "tp", axis=0, tiled=False)
    low, high = near(low), near(high)
    scale = call(scale_kernel, "scale", pltpu.VMEM((rows, 128), F32), vmem(2), (low, high))
    payload = call(
        hidden_kernel,
        "hidden",
        plain((4, rows + 512, 128), BF),
        vmem(4),
        (low, high, scale, weights),
    )
    payload = near(lax.all_to_all(payload, "tp", 0, 0, tiled=True))
    result = call(expert_kernel, "expert", plain((fs, 4, SLOTS * 128), BF), vmem(1), (payload,))
    back = near(lax.all_to_all(result, "fs", 0, 0, tiled=True))

    shares = call(
        share_kernel, "share", pltpu.VMEM((2 * count, rows), BF), vmem(2), (routes, route_weight)
    )
    mixed = call(mix_kernel, "mix", plain((count, 512), BF), vmem(2), (shares, back))
    part = plain((fs, 16, 128), BF)
    gate_out, up_out, down_out = call(
        place_kernel, "place", (part, part, plain((128, fs * 16), BF)), vmem(1), (weights,)
    )
    wide = (1, fs * 16, 128)
    return (gate_out.reshape(wide), up_out.reshape(wide), down_out[None], mixed)


def solution(mesh):
    in_specs = (
        P("fs", "tp"),
        P("fs", None),
        P("fs", None),
        P("fs"),
        P(None, "fs", "tp"),
        P(None, "fs", "tp"),
        P(None, "tp", "fs"),
    )
    out_specs = (P("fs", None, "tp"), P("fs", None, "tp"), P("fs", "tp", None), P("fs", "tp"))
    return jax.shard_map(local, mesh=mesh, in_specs=in_specs, out_specs=out_specs, check_vma=False)
```

```python
import jax
import jax.numpy as jnp
from jax import lax
from jax.experimental import pallas as pl
from jax.experimental.pallas import tpu as pltpu
from jax.sharding import PartitionSpec as P

SLOTS = 3
BF = jnp.bfloat16
F32 = jnp.float32


LIMIT = pltpu.CompilerParams(vmem_limit_bytes=12 * 2**20)


def vmem(count):
    return [pl.BlockSpec(memory_space=pltpu.VMEM)] * count


def near(value):
    return pltpu.with_memory_space_constraint(value, pltpu.VMEM)


def far(value):
    return pltpu.with_memory_space_constraint(value, pltpu.HBM)


def slot_hits(routes):
    experts = lax.axis_size("fs")
    count = routes.shape[1]
    expert = lax.broadcasted_iota(jnp.int32, (experts, count), 0)
    first = routes[0:1, :] == expert
    second = routes[1:2, :] == expert
    hit = jnp.where(first | second, 1.0, 0.0)
    before = lax.broadcasted_iota(jnp.int32, (count, count), 0) < lax.broadcasted_iota(
        jnp.int32, (count, count), 1
    )
    order = jnp.dot(hit.astype(BF), jnp.where(before, 1.0, 0.0).astype(BF), preferred_element_type=F32)
    return first, hit, order


def pack_kernel(routes_ref, tokens_ref, out_ref, rows_ref, sems):
    _, hit, order = slot_hits(routes_ref[...])
    tokens = tokens_ref[...]
    step = rows_ref.shape[0] // 2
    chosen = [jnp.where((hit > 0.0) & (order == float(s)), 1.0, 0.0).astype(BF) for s in range(SLOTS)]
    copies = []
    for h in range(2):
        piece = slice(h * step, (h + 1) * step)
        rows = jnp.dot(
            jnp.concatenate([c[piece] for c in chosen], axis=0), tokens, preferred_element_type=F32
        )
        for s in range(SLOTS):
            part = rows[s * step : (s + 1) * step].reshape(step, 4, 128)
            rows_ref[piece, :, s * 128 : (s + 1) * 128] = part.astype(BF)
        copies.append(pltpu.make_async_copy(rows_ref.at[piece], out_ref.at[piece], sems.at[h]))
        copies[-1].start()
    for copy in copies:
        copy.wait()


def cast_kernel(core_ref, gate_ref, up_ref, down_ref, gain_ref, keep_ref, send_ref):
    gain = gain_ref[...][None]
    for target, core in ((keep_ref, core_ref[0]), (send_ref, 1 - core_ref[0])):
        target[:, :16, :] = (gate_ref[:, core] * gain).astype(BF)
        target[:, 16:32, :] = (up_ref[:, core] * gain).astype(BF)
        target[:, 32:, :] = down_ref[:, core].astype(BF)


def join_kernel(core_ref, keep_ref, other_ref, out_ref):
    out_ref[:, core_ref[0]] = keep_ref[...]
    out_ref[:, 1 - core_ref[0]] = other_ref[...]


def unpack_kernel(got_ref, low_ref, high_ref):
    sources = got_ref.shape[0]
    half = low_ref.shape[0]
    blocks = []
    for s in range(SLOTS):
        block = got_ref[:, :, s * 128 : (s + 1) * 128].astype(F32)
        blocks.append(block.reshape(sources, 512).astype(BF))
    low_ref[:sources, :] = blocks[0]
    low_ref[sources:, :] = blocks[1][: half - sources, :]
    high_ref[: 2 * sources - half, :] = blocks[1][half - sources :, :]
    high_ref[2 * sources - half :, :] = blocks[2]


def place_kernel(weight_ref, gate_ref, up_ref, down_ref):
    gate_ref[...] = weight_ref[:, :16, :]
    up_ref[...] = weight_ref[:, 16:32, :]
    block = weight_ref[:, 32:, :].reshape(weight_ref.shape[0] * 16, 128)
    down_ref[...] = block.astype(F32).T.astype(BF)


def scale_kernel(low_ref, high_ref, out_ref):
    half = low_ref.shape[1]
    for h, ref in enumerate((low_ref, high_ref)):
        total = None
        for k in range(4):
            value = ref[k].astype(F32)
            part = jnp.sum(value * value, axis=1, keepdims=True)
            total = part if total is None else total + part
        scale = lax.rsqrt(total / 2048.0 + 1e-06)
        out_ref[h * half : (h + 1) * half, :] = jnp.broadcast_to(scale, (half, 128))


def hidden_kernel(low_ref, high_ref, scale_ref, weight_ref, out_ref):
    half = low_ref.shape[1]
    total = 2 * half
    part = weight_ref.shape[0] // 4

    def block(k, kind):
        piece = weight_ref[k * part : (k + 1) * part, 16 * kind : 16 * kind + 16, :]
        return piece.reshape(part * 16, 128)

    accs = [None, None]
    for k in range(4):
        weight = jnp.concatenate((block(k, 0), block(k, 1)), axis=1)
        for h, ref in enumerate((low_ref, high_ref)):
            product = jnp.dot(ref[k], weight, preferred_element_type=F32)
            accs[h] = product if k == 0 else accs[h] + product
        out_ref[k, total:, :] = block(k, 2)
    for h in range(2):
        scale = scale_ref[h * half : (h + 1) * half, :]
        gate = accs[h][:, :128] * scale
        up = accs[h][:, 128:] * scale
        hidden = (gate / (1.0 + jnp.exp(-gate)) * up).astype(BF)
        for k in range(4):
            out_ref[k, h * half : (h + 1) * half, :] = hidden


def expert_kernel(got_ref, out_ref):
    sources = out_ref.shape[0]
    total = SLOTS * sources
    result = lax.dot_general(
        jnp.concatenate([got_ref[k, :total, :] for k in range(4)], axis=1),
        jnp.concatenate([got_ref[k, total:, :] for k in range(4)], axis=1),
        (((1,), (1,)), ((), ())),
        preferred_element_type=F32,
    )
    for s in range(SLOTS):
        rows = result[s * sources : (s + 1) * sources, :]
        out_ref[:, :, s * 128 : (s + 1) * 128] = rows.reshape(sources, 4, 128).astype(BF)


def share_kernel(routes_ref, weight_ref, out_ref):
    first, hit, order = slot_hits(routes_ref[...])
    weight = weight_ref[...]
    share = weight / jnp.sum(weight, axis=0, keepdims=True)
    mine = jnp.where(first, share[0:1, :], share[1:2, :])
    count = out_ref.shape[0] // 2
    for s in range(SLOTS):
        part = jnp.where((hit > 0.0) & (order == float(s)), mine, 0.0).T
        high = part.astype(BF)
        columns = slice(s * part.shape[1], (s + 1) * part.shape[1])
        out_ref[:count, columns] = high
        out_ref[count:, columns] = (part - high.astype(F32)).astype(BF)


def mix_kernel(share_ref, back_ref, out_ref):
    experts = back_ref.shape[0]
    blocks = []
    for s in range(SLOTS):
        block = back_ref[:, :, s * 128 : (s + 1) * 128].astype(F32)
        blocks.append(block.reshape(experts, 512).astype(BF))
    both = jnp.dot(share_ref[...], jnp.concatenate(blocks, axis=0), preferred_element_type=F32)
    count = out_ref.shape[0]
    out_ref[...] = (both[:count] + both[count:]).astype(BF)


def call(kernel, outs, in_specs, args, scratch=()):
    many = isinstance(outs, tuple)
    return pl.pallas_call(
        kernel,
        out_shape=outs,
        in_specs=in_specs,
        out_specs=tuple(vmem(len(outs))) if many else vmem(1)[0],
        scratch_shapes=scratch,
        compiler_params=LIMIT,
    )(*args)


def local(tokens, routes, route_weight, gain, gate_weight, up_weight, down_weight):
    fs = lax.axis_size("fs")
    count = tokens.shape[0]
    rows = SLOTS * fs
    plain = jax.ShapeDtypeStruct
    routes = routes.T
    route_weight = route_weight.T

    slots = (fs, 4, SLOTS * 128)
    packed = pl.pallas_call(
        pack_kernel,
        out_shape=plain(slots, BF),
        in_specs=vmem(2),
        out_specs=pl.BlockSpec(memory_space=pltpu.HBM),
        scratch_shapes=[pltpu.VMEM(slots, BF), pltpu.SemaphoreType.DMA((2,))],
        compiler_params=LIMIT,
        name="pack",
    )(far(routes), far(tokens))
    got = lax.all_to_all(packed, "fs", 0, 0, tiled=True)
    got = near(got)

    scalar = [pl.BlockSpec(memory_space=pltpu.SMEM)]
    core = (lax.axis_index("fs") % 2).astype(jnp.int32).reshape(1)
    chips = fs // 2
    by_chip = (chips, 2, 16, 128)
    keep, send = call(
        cast_kernel,
        (plain((chips, 48, 128), BF),) * 2,
        scalar + vmem(4),
        (
            core,
            far(gate_weight.reshape(by_chip)),
            far(up_weight.reshape(by_chip)),
            far(jnp.transpose(down_weight, (0, 2, 1)).reshape(by_chip)),
            jnp.broadcast_to(gain[:, None], (16, 128)),
        ),
    )
    other = lax.ppermute(send, "fs", [(i, i ^ 1) for i in range(fs)])
    joined = call(
        join_kernel, plain((chips, 2, 48, 128), BF), scalar + vmem(2), (core, keep, other)
    )
    same_core = [[2 * m + c for m in range(chips)] for c in range(2)]
    weights = lax.all_to_all(joined, "fs", 0, 0, tiled=True, axis_index_groups=same_core)
    weights = near(weights.reshape(fs, 48, 128))

    part = pltpu.VMEM((rows // 2, 512), BF)
    low, high = call(unpack_kernel, (part, part), vmem(1), (got,))
    low = lax.all_gather(low, "tp", axis=0, tiled=False)
    low, high = lax.optimization_barrier((low, high))
    high = lax.all_gather(high, "tp", axis=0, tiled=False)
    low, high = near(low), near(high)
    scale = call(scale_kernel, pltpu.VMEM((rows, 128), F32), vmem(2), (low, high))
    payload = call(
        hidden_kernel, plain((4, rows + 512, 128), BF), vmem(4), (low, high, scale, weights)
    )
    payload = near(lax.all_to_all(payload, "tp", 0, 0, tiled=True))
    result = call(expert_kernel, plain((fs, 4, SLOTS * 128), BF), vmem(1), (payload,))
    back = near(lax.all_to_all(result, "fs", 0, 0, tiled=True))

    shares = call(share_kernel, pltpu.VMEM((2 * count, rows), BF), vmem(2), (routes, route_weight))
    mixed = call(mix_kernel, plain((count, 512), BF), vmem(2), (shares, back))
    part = plain((fs, 16, 128), BF)
    gate_out, up_out, down_out = call(
        place_kernel, (part, part, plain((128, fs * 16), BF)), vmem(1), (weights,)
    )
    wide = (1, fs * 16, 128)
    return (gate_out.reshape(wide), up_out.reshape(wide), down_out[None], mixed)


def solution(mesh):
    in_specs = (
        P("fs", "tp"),
        P("fs", None),
        P("fs", None),
        P("fs"),
        P(None, "fs", "tp"),
        P(None, "fs", "tp"),
        P(None, "tp", "fs"),
    )
    out_specs = (P("fs", None, "tp"), P("fs", None, "tp"), P("fs", "tp", None), P("fs", "tp"))

    return jax.shard_map(local, mesh=mesh, in_specs=in_specs, out_specs=out_specs, check_vma=False)
```

```python
import jax
import jax.numpy as jnp
from jax import lax
from jax.experimental import pallas as pl
from jax.experimental.pallas import tpu as pltpu
from jax.sharding import PartitionSpec as P

SLOTS = 3
BF = jnp.bfloat16
F32 = jnp.float32


LIMIT = pltpu.CompilerParams(vmem_limit_bytes=12 * 2**20)


def vmem(count):
    return [pl.BlockSpec(memory_space=pltpu.VMEM)] * count


def near(value):
    return pltpu.with_memory_space_constraint(value, pltpu.VMEM)


def far(value):
    return pltpu.with_memory_space_constraint(value, pltpu.HBM)


def slot_hits(routes):
    experts = lax.axis_size("fs")
    count = routes.shape[1]
    expert = lax.broadcasted_iota(jnp.int32, (experts, count), 0)
    first = routes[0:1, :] == expert
    second = routes[1:2, :] == expert
    hit = jnp.where(first | second, 1.0, 0.0)
    before = lax.broadcasted_iota(jnp.int32, (count, count), 0) < lax.broadcasted_iota(
        jnp.int32, (count, count), 1
    )
    order = jnp.dot(hit.astype(BF), jnp.where(before, 1.0, 0.0).astype(BF), preferred_element_type=F32)
    return first, hit, order


def pack_kernel(routes_ref, tokens_ref, out_ref, rows_ref, sems):
    _, hit, order = slot_hits(routes_ref[...])
    tokens = tokens_ref[...]
    step = rows_ref.shape[0] // 2
    chosen = [jnp.where((hit > 0.0) & (order == float(s)), 1.0, 0.0).astype(BF) for s in range(SLOTS)]
    copies = []
    for h in range(2):
        piece = slice(h * step, (h + 1) * step)
        rows = jnp.dot(
            jnp.concatenate([c[piece] for c in chosen], axis=0), tokens, preferred_element_type=F32
        )
        for s in range(SLOTS):
            part = rows[s * step : (s + 1) * step].reshape(step, 4, 128)
            rows_ref[piece, :, s * 128 : (s + 1) * 128] = part.astype(BF)
        copies.append(pltpu.make_async_copy(rows_ref.at[piece], out_ref.at[piece], sems.at[h]))
        copies[-1].start()
    for copy in copies:
        copy.wait()


def cast_kernel(core_ref, gate_ref, up_ref, down_ref, gain_ref, keep_ref, send_ref):
    gain = gain_ref[...][None]
    for target, core in ((keep_ref, core_ref[0]), (send_ref, 1 - core_ref[0])):
        target[:, :16, :] = (gate_ref[:, core] * gain).astype(BF)
        target[:, 16:32, :] = (up_ref[:, core] * gain).astype(BF)
        target[:, 32:, :] = down_ref[:, core].astype(BF)


def join_kernel(core_ref, keep_ref, other_ref, out_ref):
    out_ref[:, core_ref[0]] = keep_ref[...]
    out_ref[:, 1 - core_ref[0]] = other_ref[...]


def unpack_kernel(got_ref, low_ref, high_ref):
    sources = got_ref.shape[0]
    half = low_ref.shape[0]
    blocks = []
    for s in range(SLOTS):
        block = got_ref[:, :, s * 128 : (s + 1) * 128].astype(F32)
        blocks.append(block.reshape(sources, 512).astype(BF))
    low_ref[:sources, :] = blocks[0]
    low_ref[sources:, :] = blocks[1][: half - sources, :]
    high_ref[: 2 * sources - half, :] = blocks[1][half - sources :, :]
    high_ref[2 * sources - half :, :] = blocks[2]


def place_kernel(weight_ref, gate_ref, up_ref, down_ref):
    gate_ref[...] = weight_ref[:, :16, :]
    up_ref[...] = weight_ref[:, 16:32, :]
    block = weight_ref[:, 32:, :].reshape(weight_ref.shape[0] * 16, 128)
    down_ref[...] = block.astype(F32).T.astype(BF)


def scale_kernel(low_ref, high_ref, out_ref):
    half = low_ref.shape[1]
    for h, ref in enumerate((low_ref, high_ref)):
        total = None
        for k in range(4):
            value = ref[k].astype(F32)
            part = jnp.sum(value * value, axis=1, keepdims=True)
            total = part if total is None else total + part
        scale = lax.rsqrt(total / 2048.0 + 1e-06)
        out_ref[h * half : (h + 1) * half, :] = jnp.broadcast_to(scale, (half, 128))


def hidden_kernel(low_ref, high_ref, scale_ref, weight_ref, out_ref):
    half = low_ref.shape[1]
    total = 2 * half
    part = weight_ref.shape[0] // 4

    def block(k, kind):
        piece = weight_ref[k * part : (k + 1) * part, 16 * kind : 16 * kind + 16, :]
        return piece.reshape(part * 16, 128)

    accs = [None, None]
    for k in range(4):
        weight = jnp.concatenate((block(k, 0), block(k, 1)), axis=1)
        for h, ref in enumerate((low_ref, high_ref)):
            product = jnp.dot(ref[k], weight, preferred_element_type=F32)
            accs[h] = product if k == 0 else accs[h] + product
        out_ref[k, total:, :] = block(k, 2)
    for h in range(2):
        scale = scale_ref[h * half : (h + 1) * half, :]
        gate = accs[h][:, :128] * scale
        up = accs[h][:, 128:] * scale
        hidden = (gate / (1.0 + jnp.exp(-gate)) * up).astype(BF)
        for k in range(4):
            out_ref[k, h * half : (h + 1) * half, :] = hidden


def expert_kernel(core_ref, got_ref, keep_ref, send_ref):
    chips = keep_ref.shape[0]
    sources = 2 * chips
    first = core_ref[0] == 0
    total = SLOTS * sources
    result = lax.dot_general(
        jnp.concatenate([got_ref[k, :total, :] for k in range(4)], axis=1),
        jnp.concatenate([got_ref[k, total:, :] for k in range(4)], axis=1),
        (((1,), (1,)), ((), ())),
        preferred_element_type=F32,
    )
    for s in range(SLOTS):
        rows = result[s * sources : (s + 1) * sources, :].reshape(chips, 2, 4, 128)
        columns = slice(s * 128, (s + 1) * 128)
        keep_ref[:, :, columns] = jnp.where(first, rows[:, 0], rows[:, 1]).astype(BF)
        send_ref[:, :, columns] = jnp.where(first, rows[:, 1], rows[:, 0]).astype(BF)


def share_kernel(routes_ref, weight_ref, out_ref):
    first, hit, order = slot_hits(routes_ref[...])
    weight = weight_ref[...]
    share = weight / jnp.sum(weight, axis=0, keepdims=True)
    mine = jnp.where(first, share[0:1, :], share[1:2, :])
    count = out_ref.shape[0] // 2
    for s in range(SLOTS):
        part = jnp.where((hit > 0.0) & (order == float(s)), mine, 0.0).T
        high = part.astype(BF)
        columns = slice(s * part.shape[1], (s + 1) * part.shape[1])
        out_ref[:count, columns] = high
        out_ref[count:, columns] = (part - high.astype(F32)).astype(BF)


def mix_kernel(share_ref, back_ref, out_ref):
    experts = back_ref.shape[0]
    blocks = []
    for s in range(SLOTS):
        block = back_ref[:, :, s * 128 : (s + 1) * 128].astype(F32)
        blocks.append(block.reshape(experts, 512).astype(BF))
    both = jnp.dot(share_ref[...], jnp.concatenate(blocks, axis=0), preferred_element_type=F32)
    count = out_ref.shape[0]
    out_ref[...] = (both[:count] + both[count:]).astype(BF)


def call(kernel, outs, in_specs, args, scratch=()):
    many = isinstance(outs, tuple)
    return pl.pallas_call(
        kernel,
        out_shape=outs,
        in_specs=in_specs,
        out_specs=tuple(vmem(len(outs))) if many else vmem(1)[0],
        scratch_shapes=scratch,
        compiler_params=LIMIT,
    )(*args)


def local(tokens, routes, route_weight, gain, gate_weight, up_weight, down_weight):
    fs = lax.axis_size("fs")
    count = tokens.shape[0]
    rows = SLOTS * fs
    plain = jax.ShapeDtypeStruct
    routes = routes.T
    route_weight = route_weight.T

    slots = (fs, 4, SLOTS * 128)
    packed = pl.pallas_call(
        pack_kernel,
        out_shape=plain(slots, BF),
        in_specs=vmem(2),
        out_specs=pl.BlockSpec(memory_space=pltpu.HBM),
        scratch_shapes=[pltpu.VMEM(slots, BF), pltpu.SemaphoreType.DMA((2,))],
        compiler_params=LIMIT,
        name="pack",
    )(far(routes), far(tokens))
    got = lax.all_to_all(packed, "fs", 0, 0, tiled=True)
    got = near(got)

    scalar = [pl.BlockSpec(memory_space=pltpu.SMEM)]
    core = (lax.axis_index("fs") % 2).astype(jnp.int32).reshape(1)
    chips = fs // 2
    by_chip = (chips, 2, 16, 128)
    keep, send = call(
        cast_kernel,
        (plain((chips, 48, 128), BF),) * 2,
        scalar + vmem(4),
        (
            core,
            far(gate_weight.reshape(by_chip)),
            far(up_weight.reshape(by_chip)),
            far(jnp.transpose(down_weight, (0, 2, 1)).reshape(by_chip)),
            jnp.broadcast_to(gain[:, None], (16, 128)),
        ),
    )
    other = lax.ppermute(send, "fs", [(i, i ^ 1) for i in range(fs)])
    joined = call(
        join_kernel, plain((chips, 2, 48, 128), BF), scalar + vmem(2), (core, keep, other)
    )
    same_core = [[2 * m + c for m in range(chips)] for c in range(2)]
    weights = lax.all_to_all(joined, "fs", 0, 0, tiled=True, axis_index_groups=same_core)
    weights = near(weights.reshape(fs, 48, 128))

    part = pltpu.VMEM((rows // 2, 512), BF)
    low, high = call(unpack_kernel, (part, part), vmem(1), (got,))
    low = lax.all_gather(low, "tp", axis=0, tiled=False)
    low, high = lax.optimization_barrier((low, high))
    high = lax.all_gather(high, "tp", axis=0, tiled=False)
    low, high = near(low), near(high)
    scale = call(scale_kernel, pltpu.VMEM((rows, 128), F32), vmem(2), (low, high))
    payload = call(
        hidden_kernel, plain((4, rows + 512, 128), BF), vmem(4), (low, high, scale, weights)
    )
    payload = near(lax.all_to_all(payload, "tp", 0, 0, tiled=True))
    piece = pltpu.VMEM((chips, 4, SLOTS * 128), BF)
    keep, send = call(expert_kernel, (piece, piece), scalar + vmem(1), (core, payload))
    other = near(lax.ppermute(send, "fs", [(i, i ^ 1) for i in range(fs)]))
    joined = call(
        join_kernel, plain((chips, 2, 4, SLOTS * 128), BF), scalar + vmem(2), (core, keep, other)
    )
    back = lax.all_to_all(joined, "fs", 0, 0, tiled=True, axis_index_groups=same_core)
    back = near(back.reshape(fs, 4, SLOTS * 128))

    shares = call(share_kernel, pltpu.VMEM((2 * count, rows), BF), vmem(2), (routes, route_weight))
    mixed = call(mix_kernel, plain((count, 512), BF), vmem(2), (shares, back))
    part = plain((fs, 16, 128), BF)
    gate_out, up_out, down_out = call(
        place_kernel, (part, part, plain((128, fs * 16), BF)), vmem(1), (weights,)
    )
    wide = (1, fs * 16, 128)
    return (gate_out.reshape(wide), up_out.reshape(wide), down_out[None], mixed)


def solution(mesh):
    in_specs = (
        P("fs", "tp"),
        P("fs", None),
        P("fs", None),
        P("fs"),
        P(None, "fs", "tp"),
        P(None, "fs", "tp"),
        P(None, "tp", "fs"),
    )
    out_specs = (P("fs", None, "tp"), P("fs", None, "tp"), P("fs", "tp", None), P("fs", "tp"))

    return jax.shard_map(local, mesh=mesh, in_specs=in_specs, out_specs=out_specs, check_vma=False)
```

```python
import jax
import jax.numpy as jnp
from jax import lax
from jax.experimental import pallas as pl
from jax.experimental.pallas import tpu as pltpu
from jax.sharding import PartitionSpec as P

SLOTS = 3
BF = jnp.bfloat16
F32 = jnp.float32


LIMIT = pltpu.CompilerParams(vmem_limit_bytes=12 * 2**20)


def vmem(count):
    return [pl.BlockSpec(memory_space=pltpu.VMEM)] * count


def near(value):
    return pltpu.with_memory_space_constraint(value, pltpu.VMEM)


def far(value):
    return pltpu.with_memory_space_constraint(value, pltpu.HBM)


def slot_hits(routes):
    experts = lax.axis_size("fs")
    count = routes.shape[1]
    expert = lax.broadcasted_iota(jnp.int32, (experts, count), 0)
    first = routes[0:1, :] == expert
    second = routes[1:2, :] == expert
    hit = jnp.where(first | second, 1.0, 0.0)
    before = lax.broadcasted_iota(jnp.int32, (count, count), 0) < lax.broadcasted_iota(
        jnp.int32, (count, count), 1
    )
    order = jnp.dot(hit.astype(BF), jnp.where(before, 1.0, 0.0).astype(BF), preferred_element_type=F32)
    return first, hit, order


def pack_kernel(routes_ref, tokens_ref, out_ref, rows_ref, sems):
    _, hit, order = slot_hits(routes_ref[...])
    tokens = tokens_ref[...]
    step = rows_ref.shape[0] // 2
    chosen = [jnp.where((hit > 0.0) & (order == float(s)), 1.0, 0.0).astype(BF) for s in range(SLOTS)]
    copies = []
    for h in range(2):
        piece = slice(h * step, (h + 1) * step)
        rows = jnp.dot(
            jnp.concatenate([c[piece] for c in chosen], axis=0), tokens, preferred_element_type=F32
        )
        for s in range(SLOTS):
            part = rows[s * step : (s + 1) * step].reshape(step, 4, 128)
            rows_ref[piece, :, s * 128 : (s + 1) * 128] = part.astype(BF)
        copies.append(pltpu.make_async_copy(rows_ref.at[piece], out_ref.at[piece], sems.at[h]))
        copies[-1].start()
    for copy in copies:
        copy.wait()


def cast_kernel(core_ref, gate_ref, up_ref, down_ref, gain_ref, keep_ref, send_ref):
    gain = gain_ref[...][None]
    for target, core in ((keep_ref, core_ref[0]), (send_ref, 1 - core_ref[0])):
        target[:, :16, :] = (gate_ref[:, core] * gain).astype(BF)
        target[:, 16:32, :] = (up_ref[:, core] * gain).astype(BF)
        target[:, 32:, :] = down_ref[:, core].astype(BF)


def join_kernel(core_ref, keep_ref, other_ref, out_ref):
    out_ref[:, core_ref[0]] = keep_ref[...]
    out_ref[:, 1 - core_ref[0]] = other_ref[...]


def unpack_kernel(got_ref, low_ref, high_ref):
    sources = got_ref.shape[0]
    half = low_ref.shape[0]
    blocks = []
    for s in range(SLOTS):
        block = got_ref[:, :, s * 128 : (s + 1) * 128].astype(F32)
        blocks.append(block.reshape(sources, 512).astype(BF))
    low_ref[:sources, :] = blocks[0]
    low_ref[sources:, :] = blocks[1][: half - sources, :]
    high_ref[: 2 * sources - half, :] = blocks[1][half - sources :, :]
    high_ref[2 * sources - half :, :] = blocks[2]


def scale_kernel(low_ref, high_ref, out_ref):
    half = low_ref.shape[1]
    for h, ref in enumerate((low_ref, high_ref)):
        total = None
        for k in range(4):
            value = ref[k].astype(F32)
            part = jnp.sum(value * value, axis=1, keepdims=True)
            total = part if total is None else total + part
        scale = lax.rsqrt(total / 2048.0 + 1e-06)
        out_ref[h * half : (h + 1) * half, :] = jnp.broadcast_to(scale, (half, 128))


def hidden_kernel(low_ref, high_ref, scale_ref, weight_ref, out_ref):
    half = low_ref.shape[1]
    total = 2 * half
    part = weight_ref.shape[0] // 4

    def block(k, kind):
        piece = weight_ref[k * part : (k + 1) * part, 16 * kind : 16 * kind + 16, :]
        return piece.reshape(part * 16, 128)

    accs = [None, None]
    for k in range(4):
        weight = jnp.concatenate((block(k, 0), block(k, 1)), axis=1)
        for h, ref in enumerate((low_ref, high_ref)):
            product = jnp.dot(ref[k], weight, preferred_element_type=F32)
            accs[h] = product if k == 0 else accs[h] + product
        out_ref[k, total:, :] = block(k, 2)
    for h in range(2):
        scale = scale_ref[h * half : (h + 1) * half, :]
        gate = accs[h][:, :128] * scale
        up = accs[h][:, 128:] * scale
        hidden = (gate / (1.0 + jnp.exp(-gate)) * up).astype(BF)
        for k in range(4):
            out_ref[k, h * half : (h + 1) * half, :] = hidden


def expert_kernel(got_ref, weight_ref, out_ref, gate_hbm, up_hbm, sems):
    copies = [
        pltpu.make_async_copy(weight_ref.at[:, pl.ds(16 * k, 16), :], ref, sems.at[k])
        for k, ref in enumerate((gate_hbm, up_hbm))
    ]
    for copy in copies:
        copy.start()
    sources = out_ref.shape[0]
    total = SLOTS * sources
    result = lax.dot_general(
        jnp.concatenate([got_ref[k, :total, :] for k in range(4)], axis=1),
        jnp.concatenate([got_ref[k, total:, :] for k in range(4)], axis=1),
        (((1,), (1,)), ((), ())),
        preferred_element_type=F32,
    )
    for s in range(SLOTS):
        rows = result[s * sources : (s + 1) * sources, :]
        out_ref[:, :, s * 128 : (s + 1) * 128] = rows.reshape(sources, 4, 128).astype(BF)
    for copy in copies:
        copy.wait()


def share_kernel(routes_ref, weight_ref, out_ref):
    first, hit, order = slot_hits(routes_ref[...])
    weight = weight_ref[...]
    share = weight / jnp.sum(weight, axis=0, keepdims=True)
    mine = jnp.where(first, share[0:1, :], share[1:2, :])
    count = out_ref.shape[0] // 2
    for s in range(SLOTS):
        part = jnp.where((hit > 0.0) & (order == float(s)), mine, 0.0).T
        high = part.astype(BF)
        columns = slice(s * part.shape[1], (s + 1) * part.shape[1])
        out_ref[:count, columns] = high
        out_ref[count:, columns] = (part - high.astype(F32)).astype(BF)


def mix_kernel(share_ref, back_ref, weight_ref, out_ref, down_ref):
    experts = back_ref.shape[0]
    blocks = []
    for s in range(SLOTS):
        block = back_ref[:, :, s * 128 : (s + 1) * 128].astype(F32)
        blocks.append(block.reshape(experts, 512).astype(BF))
    both = jnp.dot(share_ref[...], jnp.concatenate(blocks, axis=0), preferred_element_type=F32)
    count = out_ref.shape[0]
    out_ref[...] = (both[:count] + both[count:]).astype(BF)
    down = weight_ref[:, 32:, :].reshape(weight_ref.shape[0] * 16, 128)
    down_ref[...] = down.astype(F32).T.astype(BF)


def call(kernel, outs, in_specs, args, scratch=()):
    many = isinstance(outs, tuple)
    return pl.pallas_call(
        kernel,
        out_shape=outs,
        in_specs=in_specs,
        out_specs=tuple(vmem(len(outs))) if many else vmem(1)[0],
        scratch_shapes=scratch,
        compiler_params=LIMIT,
    )(*args)


def local(tokens, routes, route_weight, gain, gate_weight, up_weight, down_weight):
    fs = lax.axis_size("fs")
    count = tokens.shape[0]
    rows = SLOTS * fs
    plain = jax.ShapeDtypeStruct
    routes = routes.T
    route_weight = route_weight.T

    slots = (fs, 4, SLOTS * 128)
    packed = pl.pallas_call(
        pack_kernel,
        out_shape=plain(slots, BF),
        in_specs=vmem(2),
        out_specs=pl.BlockSpec(memory_space=pltpu.HBM),
        scratch_shapes=[pltpu.VMEM(slots, BF), pltpu.SemaphoreType.DMA((2,))],
        compiler_params=LIMIT,
        name="pack",
    )(far(routes), far(tokens))
    got = lax.all_to_all(packed, "fs", 0, 0, tiled=True)
    got = near(got)

    scalar = [pl.BlockSpec(memory_space=pltpu.SMEM)]
    core = (lax.axis_index("fs") % 2).astype(jnp.int32).reshape(1)
    chips = fs // 2
    by_chip = (chips, 2, 16, 128)
    keep, send = call(
        cast_kernel,
        (plain((chips, 48, 128), BF),) * 2,
        scalar + vmem(4),
        (
            core,
            far(gate_weight.reshape(by_chip)),
            far(up_weight.reshape(by_chip)),
            far(jnp.transpose(down_weight, (0, 2, 1)).reshape(by_chip)),
            jnp.broadcast_to(gain[:, None], (16, 128)),
        ),
    )
    other = lax.ppermute(send, "fs", [(i, i ^ 1) for i in range(fs)])
    joined = call(
        join_kernel, plain((chips, 2, 48, 128), BF), scalar + vmem(2), (core, keep, other)
    )
    same_core = [[2 * m + c for m in range(chips)] for c in range(2)]
    weights = lax.all_to_all(joined, "fs", 0, 0, tiled=True, axis_index_groups=same_core)
    weights = near(weights.reshape(fs, 48, 128))

    part = pltpu.VMEM((rows // 2, 512), BF)
    low, high = call(unpack_kernel, (part, part), vmem(1), (got,))
    low = lax.all_gather(low, "tp", axis=0, tiled=False)
    low, high = lax.optimization_barrier((low, high))
    high = lax.all_gather(high, "tp", axis=0, tiled=False)
    low, high = near(low), near(high)
    scale = call(scale_kernel, pltpu.VMEM((rows, 128), F32), vmem(2), (low, high))
    payload = call(
        hidden_kernel, plain((4, rows + 512, 128), BF), vmem(4), (low, high, scale, weights)
    )
    payload = near(lax.all_to_all(payload, "tp", 0, 0, tiled=True))
    part = plain((fs, 16, 128), BF)
    hbm = pl.BlockSpec(memory_space=pltpu.HBM)
    result, gate_out, up_out = pl.pallas_call(
        expert_kernel,
        out_shape=(pltpu.VMEM((fs, 4, SLOTS * 128), BF), part, part),
        in_specs=vmem(2),
        out_specs=(vmem(1)[0], hbm, hbm),
        scratch_shapes=[pltpu.SemaphoreType.DMA((2,))],
        compiler_params=LIMIT,
        name="expert",
    )(payload, weights)
    back = near(lax.all_to_all(result, "fs", 0, 0, tiled=True))

    shares = call(
        share_kernel, pltpu.VMEM((2 * count, rows), BF), vmem(2), (far(routes), far(route_weight))
    )
    mixed, down_out = call(
        mix_kernel,
        (plain((count, 512), BF), plain((128, fs * 16), BF)),
        vmem(3),
        (shares, back, weights),
    )
    wide = (1, fs * 16, 128)
    return (gate_out.reshape(wide), up_out.reshape(wide), down_out[None], mixed)


def solution(mesh):
    in_specs = (
        P("fs", "tp"),
        P("fs", None),
        P("fs", None),
        P("fs"),
        P(None, "fs", "tp"),
        P(None, "fs", "tp"),
        P(None, "tp", "fs"),
    )
    out_specs = (P("fs", None, "tp"), P("fs", None, "tp"), P("fs", "tp", None), P("fs", "tp"))

    return jax.shard_map(local, mesh=mesh, in_specs=in_specs, out_specs=out_specs, check_vma=False)
```

```python
import jax
import jax.numpy as jnp
from jax import lax
from jax.experimental import pallas as pl
from jax.experimental.pallas import tpu as pltpu
from jax.sharding import PartitionSpec as P

SLOTS = 3
BF = jnp.bfloat16
F32 = jnp.float32


LIMIT = pltpu.CompilerParams(vmem_limit_bytes=12 * 2**20)


def vmem(count):
    return [pl.BlockSpec(memory_space=pltpu.VMEM)] * count


def near(value):
    return pltpu.with_memory_space_constraint(value, pltpu.VMEM)


def far(value):
    return pltpu.with_memory_space_constraint(value, pltpu.HBM)


def slot_hits(routes):
    experts = lax.axis_size("fs")
    count = routes.shape[1]
    expert = lax.broadcasted_iota(jnp.int32, (experts, count), 0)
    first = routes[0:1, :] == expert
    second = routes[1:2, :] == expert
    hit = jnp.where(first | second, 1.0, 0.0)
    before = lax.broadcasted_iota(jnp.int32, (count, count), 0) < lax.broadcasted_iota(
        jnp.int32, (count, count), 1
    )
    order = jnp.dot(hit.astype(BF), jnp.where(before, 1.0, 0.0).astype(BF), preferred_element_type=F32)
    return first, hit, order


def pack_kernel(routes_ref, tokens_ref, out_ref, rows_ref, sems):
    _, hit, order = slot_hits(routes_ref[...])
    tokens = tokens_ref[...]
    step = rows_ref.shape[0] // 2
    chosen = [jnp.where((hit > 0.0) & (order == float(s)), 1.0, 0.0).astype(BF) for s in range(SLOTS)]
    copies = []
    for h in range(2):
        piece = slice(h * step, (h + 1) * step)
        rows = jnp.dot(
            jnp.concatenate([c[piece] for c in chosen], axis=0), tokens, preferred_element_type=F32
        )
        for s in range(SLOTS):
            part = rows[s * step : (s + 1) * step].reshape(step, 4, 128)
            rows_ref[piece, :, s * 128 : (s + 1) * 128] = part.astype(BF)
        copies.append(pltpu.make_async_copy(rows_ref.at[piece], out_ref.at[piece], sems.at[h]))
        copies[-1].start()
    for copy in copies:
        copy.wait()


def cast_kernel(core_ref, gate_ref, up_ref, down_ref, gain_ref, keep_ref, send_ref):
    gain = gain_ref[...][None]
    for target, core in ((keep_ref, core_ref[0]), (send_ref, 1 - core_ref[0])):
        target[:, :16, :] = (gate_ref[:, core] * gain).astype(BF)
        target[:, 16:32, :] = (up_ref[:, core] * gain).astype(BF)
        target[:, 32:, :] = down_ref[:, core].astype(BF)


def join_kernel(core_ref, keep_ref, other_ref, out_ref):
    out_ref[:, core_ref[0]] = keep_ref[...]
    out_ref[:, 1 - core_ref[0]] = other_ref[...]


def unpack_kernel(got_ref, low_ref, high_ref):
    sources = got_ref.shape[0]
    half = low_ref.shape[0]
    blocks = []
    for s in range(SLOTS):
        block = got_ref[:, :, s * 128 : (s + 1) * 128].astype(F32)
        blocks.append(block.reshape(sources, 512).astype(BF))
    low_ref[:sources, :] = blocks[0]
    low_ref[sources:, :] = blocks[1][: half - sources, :]
    high_ref[: 2 * sources - half, :] = blocks[1][half - sources :, :]
    high_ref[2 * sources - half :, :] = blocks[2]


def scale_kernel(low_ref, high_ref, out_ref):
    half = low_ref.shape[1]
    for h, ref in enumerate((low_ref, high_ref)):
        total = None
        for k in range(4):
            value = ref[k].astype(F32)
            part = jnp.sum(value * value, axis=1, keepdims=True)
            total = part if total is None else total + part
        scale = lax.rsqrt(total / 2048.0 + 1e-06)
        out_ref[h * half : (h + 1) * half, :] = jnp.broadcast_to(scale, (half, 128))


def hidden_kernel(low_ref, high_ref, scale_ref, weight_ref, out_ref, gate_hbm, sem):
    copy = pltpu.make_async_copy(weight_ref.at[:, pl.ds(0, 16), :], gate_hbm, sem)
    copy.start()
    half = low_ref.shape[1]
    total = 2 * half
    part = weight_ref.shape[0] // 4

    def block(k, kind):
        piece = weight_ref[k * part : (k + 1) * part, 16 * kind : 16 * kind + 16, :]
        return piece.reshape(part * 16, 128)

    accs = [None, None]
    for k in range(4):
        weight = jnp.concatenate((block(k, 0), block(k, 1)), axis=1)
        for h, ref in enumerate((low_ref, high_ref)):
            product = jnp.dot(ref[k], weight, preferred_element_type=F32)
            accs[h] = product if k == 0 else accs[h] + product
        out_ref[k, total:, :] = block(k, 2)
    for h in range(2):
        scale = scale_ref[h * half : (h + 1) * half, :]
        gate = accs[h][:, :128] * scale
        up = accs[h][:, 128:] * scale
        hidden = (gate / (1.0 + jnp.exp(-gate)) * up).astype(BF)
        for k in range(4):
            out_ref[k, h * half : (h + 1) * half, :] = hidden
    copy.wait()


def expert_kernel(got_ref, weight_ref, out_ref, up_hbm, sem):
    copy = pltpu.make_async_copy(weight_ref.at[:, pl.ds(16, 16), :], up_hbm, sem)
    copy.start()
    sources = out_ref.shape[0]
    total = SLOTS * sources
    result = lax.dot_general(
        jnp.concatenate([got_ref[k, :total, :] for k in range(4)], axis=1),
        jnp.concatenate([got_ref[k, total:, :] for k in range(4)], axis=1),
        (((1,), (1,)), ((), ())),
        preferred_element_type=F32,
    )
    for s in range(SLOTS):
        rows = result[s * sources : (s + 1) * sources, :]
        out_ref[:, :, s * 128 : (s + 1) * 128] = rows.reshape(sources, 4, 128).astype(BF)
    copy.wait()


def share_kernel(routes_ref, weight_ref, out_ref):
    first, hit, order = slot_hits(routes_ref[...])
    weight = weight_ref[...]
    share = weight / jnp.sum(weight, axis=0, keepdims=True)
    mine = jnp.where(first, share[0:1, :], share[1:2, :])
    count = out_ref.shape[0] // 2
    for s in range(SLOTS):
        part = jnp.where((hit > 0.0) & (order == float(s)), mine, 0.0).T
        high = part.astype(BF)
        columns = slice(s * part.shape[1], (s + 1) * part.shape[1])
        out_ref[:count, columns] = high
        out_ref[count:, columns] = (part - high.astype(F32)).astype(BF)


def mix_kernel(share_ref, back_ref, weight_ref, out_ref, down_hbm, down_ref, sem):
    down = weight_ref[:, 32:, :].reshape(weight_ref.shape[0] * 16, 128)
    down_ref[...] = down.astype(F32).T.astype(BF)
    copy = pltpu.make_async_copy(down_ref, down_hbm, sem)
    copy.start()
    experts = back_ref.shape[0]
    blocks = []
    for s in range(SLOTS):
        block = back_ref[:, :, s * 128 : (s + 1) * 128].astype(F32)
        blocks.append(block.reshape(experts, 512).astype(BF))
    both = jnp.dot(share_ref[...], jnp.concatenate(blocks, axis=0), preferred_element_type=F32)
    count = out_ref.shape[0]
    out_ref[...] = (both[:count] + both[count:]).astype(BF)
    copy.wait()


def call(kernel, outs, in_specs, args, scratch=()):
    many = isinstance(outs, tuple)
    return pl.pallas_call(
        kernel,
        out_shape=outs,
        in_specs=in_specs,
        out_specs=tuple(vmem(len(outs))) if many else vmem(1)[0],
        scratch_shapes=scratch,
        compiler_params=LIMIT,
    )(*args)


def local(tokens, routes, route_weight, gain, gate_weight, up_weight, down_weight):
    fs = lax.axis_size("fs")
    count = tokens.shape[0]
    rows = SLOTS * fs
    plain = jax.ShapeDtypeStruct
    routes = routes.T
    route_weight = route_weight.T

    slots = (fs, 4, SLOTS * 128)
    packed = pl.pallas_call(
        pack_kernel,
        out_shape=plain(slots, BF),
        in_specs=vmem(2),
        out_specs=pl.BlockSpec(memory_space=pltpu.HBM),
        scratch_shapes=[pltpu.VMEM(slots, BF), pltpu.SemaphoreType.DMA((2,))],
        compiler_params=LIMIT,
        name="pack",
    )(far(routes), far(tokens))
    got = lax.all_to_all(packed, "fs", 0, 0, tiled=True)
    got = near(got)

    scalar = [pl.BlockSpec(memory_space=pltpu.SMEM)]
    core = (lax.axis_index("fs") % 2).astype(jnp.int32).reshape(1)
    chips = fs // 2
    by_chip = (chips, 2, 16, 128)
    keep, send = call(
        cast_kernel,
        (plain((chips, 48, 128), BF),) * 2,
        scalar + vmem(4),
        (
            core,
            far(gate_weight.reshape(by_chip)),
            far(up_weight.reshape(by_chip)),
            far(jnp.transpose(down_weight, (0, 2, 1)).reshape(by_chip)),
            jnp.broadcast_to(gain[:, None], (16, 128)),
        ),
    )
    other = lax.ppermute(send, "fs", [(i, i ^ 1) for i in range(fs)])
    joined = call(
        join_kernel, plain((chips, 2, 48, 128), BF), scalar + vmem(2), (core, keep, other)
    )
    same_core = [[2 * m + c for m in range(chips)] for c in range(2)]
    weights = lax.all_to_all(joined, "fs", 0, 0, tiled=True, axis_index_groups=same_core)
    weights = near(weights.reshape(fs, 48, 128))

    part = pltpu.VMEM((rows // 2, 512), BF)
    low, high = call(unpack_kernel, (part, part), vmem(1), (got,))
    low = lax.all_gather(low, "tp", axis=0, tiled=False)
    low, high = lax.optimization_barrier((low, high))
    high = lax.all_gather(high, "tp", axis=0, tiled=False)
    low, high = near(low), near(high)
    scale = call(scale_kernel, pltpu.VMEM((rows, 128), F32), vmem(2), (low, high))
    part = plain((fs, 16, 128), BF)
    hbm = pl.BlockSpec(memory_space=pltpu.HBM)
    payload, gate_out = pl.pallas_call(
        hidden_kernel,
        out_shape=(plain((4, rows + 512, 128), BF), part),
        in_specs=vmem(4),
        out_specs=(vmem(1)[0], hbm),
        scratch_shapes=[pltpu.SemaphoreType.DMA],
        compiler_params=LIMIT,
        name="hidden",
    )(low, high, scale, weights)
    payload = near(lax.all_to_all(payload, "tp", 0, 0, tiled=True))
    result, up_out = pl.pallas_call(
        expert_kernel,
        out_shape=(pltpu.VMEM((fs, 4, SLOTS * 128), BF), part),
        in_specs=vmem(2),
        out_specs=(vmem(1)[0], hbm),
        scratch_shapes=[pltpu.SemaphoreType.DMA],
        compiler_params=LIMIT,
        name="expert",
    )(payload, weights)
    back = near(lax.all_to_all(result, "fs", 0, 0, tiled=True))

    shares = call(
        share_kernel, pltpu.VMEM((2 * count, rows), BF), vmem(2), (far(routes), far(route_weight))
    )
    mixed, down_out = pl.pallas_call(
        mix_kernel,
        out_shape=(plain((count, 512), BF), plain((128, fs * 16), BF)),
        in_specs=vmem(3),
        out_specs=(vmem(1)[0], hbm),
        scratch_shapes=[pltpu.VMEM((128, fs * 16), BF), pltpu.SemaphoreType.DMA],
        compiler_params=LIMIT,
        name="mix",
    )(shares, back, weights)
    wide = (1, fs * 16, 128)
    return (gate_out.reshape(wide), up_out.reshape(wide), down_out[None], mixed)


def solution(mesh):
    in_specs = (
        P("fs", "tp"),
        P("fs", None),
        P("fs", None),
        P("fs"),
        P(None, "fs", "tp"),
        P(None, "fs", "tp"),
        P(None, "tp", "fs"),
    )
    out_specs = (P("fs", None, "tp"), P("fs", None, "tp"), P("fs", "tp", None), P("fs", "tp"))

    return jax.shard_map(local, mesh=mesh, in_specs=in_specs, out_specs=out_specs, check_vma=False)
```
